512 devices in a mesh: sp: 16 (over y, x), tp: 32 (over z, core).
Axes of the slice: x: 4, y: 4, z: 16, core: 2. Of those that a mesh axis runs over, the one named last changes fastest.
Arguments:
- tokens: bfloat16 [32768, 2048], P('sp', 'tp'), may hold values from -6 to 6
- norm_gain: float32 [2048], replicated, may hold values from 0.1 to 1.9
- w_key: bfloat16 [2048, 1024], P(None, 'tp'), may hold values from -0.125 to 0.125
- w_decay: bfloat16 [2048, 1024], P(None, 'tp'), may hold values from -0.125 to 0.125
- w_value: bfloat16 [2048, 512], replicated, may hold values from -0.125 to 0.125
- decay_bias: float32 [1024], P('tp'), may hold values from 0 to 8.5
- gate_drift: float32 [32768], P('sp'), may hold values from -1 to 1
- queries: bfloat16 [1024], P('tp'), may hold values from -6 to 6
- out_gain: float32 [4, 512], P(None, 'sp'), may hold values from 0.1 to 1.9
Outputs:
- state_cache: bfloat16 [1024, 512], P('tp', 'sp')
- first_read: float32 [4, 512], P(None, 'sp')
The draws below stay inside these ranges and needn't reach their ends.
All inputs are finite; a program needn't handle non-finite values.
Results may differ from the reference program's by a relative error of at most 0.009.
Values may be sent and summed in bfloat16 or wider, within the bound.
A program may use at most 128 MiB of HBM per device.

```python
import jax
import jax.numpy as jnp
from jax import lax

D = 2048
QUERY_KEY_HEADS = 4
KEY_CHANNELS = 256
VALUE_CHANNELS = 512
SPAN = 2048
BLOCK = 128
LEN = 32768
N_SP = 16


def draw_decay_bias(key, part):
    first, second, third = jax.random.split(key, 3)
    count = QUERY_KEY_HEADS * KEY_CHANNELS
    slow = jax.random.uniform(first, (count,), jnp.float32) < 0.5
    slow_value = jnp.log(LEN / 12.0) + jax.random.uniform(second, (count,), jnp.float32, -0.5, 0.5)
    slow_value = jnp.clip(slow_value, 0.0, 8.4)
    fast_value = jax.random.uniform(third, (count,), jnp.float32, 0.0, 1.5)
    return jnp.where(slow, slow_value, fast_value).astype(jnp.float32)


def draw_gate_drift(key, part):
    first, second = jax.random.split(key, 2)
    groups = LEN // BLOCK
    values = jax.random.uniform(second, (groups,), jnp.float32, -1.0, 1.0)
    return jnp.repeat(values, BLOCK).astype(jnp.float32)


def level_of(key, shape, pieces, least, top_value):
    gain = 1.0
    for axis_at, shards_of in pieces:
        draws = jax.random.uniform(jax.random.fold_in(jax.random.fold_in(key, 6), axis_at), (shards_of,), jnp.float32, least / len(pieces), top_value / len(pieces))
        gain = gain * jnp.repeat(jnp.exp(draws), shape[axis_at] // shards_of).reshape((-1,) + (1,) * (len(shape) - 1 - axis_at))
    return gain


def scatter_about(rng, dims, spread, bound, pieces=(), kind=jnp.bfloat16):
    loudness = level_of(rng, dims, pieces, -0.22, 0.18) if pieces else 1.0
    entries = jax.random.normal(rng, dims, jnp.float32) * spread * loudness
    return jnp.minimum(jnp.maximum(entries, -bound), bound).astype(kind)


def setup_inputs(seed: int = 0) -> dict:
    key_of = jax.random.split(jax.random.key(seed), 10)
    return {
        "tokens": scatter_about(key_of[0], (LEN, D), 1.0, 6.0, ((0, 16), (1, 32))),
        "norm_gain": jnp.clip(1.0 + 0.18 * jax.random.normal(key_of[1], (D,), jnp.float32), 0.1, 1.9),
        "w_key": scatter_about(key_of[2], (D, QUERY_KEY_HEADS * KEY_CHANNELS), D ** -0.5, 0.125, ((1, 32),)),
        "w_decay": scatter_about(key_of[3], (D, QUERY_KEY_HEADS * KEY_CHANNELS), D ** -0.5, 0.125, ((1, 32),)),
        "w_value": scatter_about(key_of[4], (D, VALUE_CHANNELS), D ** -0.5, 0.125),
        "decay_bias": draw_decay_bias(jax.random.fold_in(key_of[9], 71), 0),
        "gate_drift": draw_gate_drift(jax.random.fold_in(key_of[9], 71), 0),
        "queries": scatter_about(key_of[7], (QUERY_KEY_HEADS * KEY_CHANNELS,), 1.0, 6.0, ((0, 32),)),
        "out_gain": jnp.clip(1.0 + 0.18 * jax.random.normal(key_of[8], (QUERY_KEY_HEADS, VALUE_CHANNELS), jnp.float32), 0.1, 1.9),
    }


EPS = 1e-06
GATE_NORM = 16.0

def span_state(span_rows, span_drift, norm_gain, w_key, w_decay, w_value, decay_bias):
    rows_f32 = span_rows.astype(jnp.float32)
    inverse_rms = lax.rsqrt(lax.optimization_barrier(jnp.mean(rows_f32 * rows_f32, axis=1, keepdims=True)) + EPS)
    normed = (rows_f32 * inverse_rms * norm_gain[None, :]).astype(jnp.bfloat16)
    key_proj = jnp.dot(normed, w_key, preferred_element_type=jnp.float32).astype(jnp.bfloat16)
    gate_pre = jnp.dot(normed, w_decay, preferred_element_type=jnp.float32).astype(jnp.bfloat16)
    value_proj = jnp.dot(normed, w_value, preferred_element_type=jnp.float32).astype(jnp.bfloat16)
    log_decay = jax.nn.log_sigmoid(gate_pre.astype(jnp.float32) + decay_bias[None, :] + span_drift[:, None]) / GATE_NORM
    suffix = lax.cumsum(log_decay, axis=0, reverse=True)
    weighted = (key_proj.astype(jnp.float32) * jnp.exp(suffix - log_decay)).astype(jnp.bfloat16)
    partial_value = lax.dot_general(weighted, value_proj, (((0,), (0,)), ((), ())), preferred_element_type=jnp.float32)
    return (partial_value, suffix[0])

def reference(tokens, norm_gain, w_key, w_decay, w_value, decay_bias, gate_drift, queries, out_gain):
    span_rows = tokens.reshape(N_SP, SPAN, D)
    span_drift = gate_drift.reshape(N_SP, SPAN)

    def single_span(inputs):
        return span_state(inputs[0], inputs[1], norm_gain, w_key, w_decay, w_value, decay_bias)
    partials, span_total = lax.map(single_span, (span_rows, span_drift))
    later_sum = lax.cumsum(span_total, axis=0, reverse=True) - span_total
    matrix_state = lax.optimization_barrier(jnp.sum(jnp.exp(later_sum)[:, :, None] * partials, axis=0))
    state_cache = matrix_state.astype(jnp.bfloat16)
    query_of_head = queries.astype(jnp.float32).reshape(QUERY_KEY_HEADS, KEY_CHANNELS) * KEY_CHANNELS ** (-0.5)
    summed_read = jnp.einsum('gr,grs->gs', query_of_head, matrix_state.reshape(QUERY_KEY_HEADS, KEY_CHANNELS, VALUE_CHANNELS), precision=lax.Precision.HIGHEST)
    squares = lax.optimization_barrier(jnp.mean(summed_read * summed_read, axis=1, keepdims=True))
    first_read = summed_read * lax.rsqrt(squares + EPS) * out_gain
    return (state_cache, first_read)
```

```python
import functools

import jax
import jax.numpy as jnp
from jax import lax
from jax.experimental import pallas as pl
from jax.experimental.pallas import tpu as pltpu
from jax.sharding import PartitionSpec as P

MESH = pl.DeviceIdType.MESH
EPS = 1e-06
GATE_NORM = 16.0
KEY_CHANNELS = 256
N_SP, N_TP, N_Z = 16, 32, 16
SPAN, FEATS, VALS, CH = 2048, 64, 512, 32
HALF = SPAN // 2
VT = 32
HEADS = 4
MODEL = N_TP * FEATS
TILE = 512


def column_of(row):
    n = row.shape[1]
    on_diagonal = lax.broadcasted_iota(jnp.int32, (n, n), 0) == lax.broadcasted_iota(jnp.int32, (n, n), 1)
    return jnp.sum(jnp.where(on_diagonal, jnp.broadcast_to(row, (n, n)), 0.0), axis=1, keepdims=True)


def tile_of(col, group):
    out = jnp.broadcast_to(col[0:8], (8, 128))
    for a in range(1, 4):
        out = jnp.where(group == a, jnp.broadcast_to(col[8 * a : 8 * a + 8], (8, 128)), out)
    return out


def kernel(
    x_ref, gain_ref, wk_ref, wd_ref, wv_ref, bias_ref, drift_ref, q_ref, og_ref,
    state_ref, read_ref,
    xt, wt, acc, squares, vt_bf, msg, got, read_msg, read_got, sq_msg, sq_got,
    ring_send, ring_recv, pair_send, pair_recv,
    p_send, p_recv, r_send, r_recv, s_send, s_recv,
):
    j = lax.axis_index("sp")
    t = lax.axis_index("tp")
    z, k = t // 2, t % 2
    sibling = 2 * z + 1 - k
    up = 2 * lax.rem(z + 1, N_Z) + k
    down = 2 * lax.rem(z + N_Z - 1, N_Z) + k

    barrier = pltpu.get_barrier_semaphore()
    for other in (sibling, up, down):
        pl.semaphore_signal(barrier, inc=1, device_id=(j, other), device_id_type=MESH)

    @pl.loop(1, N_SP)
    def _(o):
        pl.semaphore_signal(barrier, inc=1, device_id=(lax.rem(j + o, N_SP), t), device_id_type=MESH)

    pl.semaphore_wait(barrier, 3 + N_SP - 1)

    def rows_of(src_z, core):
        return pl.ds(pl.multiple_of((2 * src_z + core) * FEATS, FEATS), FEATS)

    def lanes_of(sub):
        return pl.ds(sub * HALF, HALF)

    def ring(way, sub, s):
        src_z = lax.rem(z - (s - 1) + 2 * N_Z, N_Z) if way == 0 else lax.rem(z + (s - 1), N_Z)
        place = xt.at[rows_of(src_z, k), lanes_of(sub)]
        if isinstance(s, int) and s == 1:
            source = x_ref.at[:, lanes_of(sub)]
        else:
            source = place
        return pltpu.make_async_remote_copy(
            src_ref=source, dst_ref=place,
            send_sem=ring_send.at[way, sub, s], recv_sem=ring_recv.at[way, sub, s],
            device_id=(j, up if way == 0 else down), device_id_type=MESH,
        )

    def pair(src_z, sub, slot, own=False):
        place = xt.at[rows_of(src_z, k), lanes_of(sub)]
        return pltpu.make_async_remote_copy(
            src_ref=x_ref.at[:, lanes_of(sub)] if own else place, dst_ref=place,
            send_sem=pair_send.at[slot, sub], recv_sem=pair_recv.at[slot, sub],
            device_id=(j, sibling), device_id_type=MESH,
        )

    for sub in range(2):
        for way in range(2):
            ring(way, sub, 1).start()
    for sub in range(2):
        pair(z, sub, 0, own=True).start()

    xt[rows_of(z, k), :] = x_ref[...]
    gain = gain_ref[...]
    wt[0:CH, :] = (wk_ref[...].astype(jnp.float32) * gain).astype(jnp.bfloat16)
    wt[CH : 2 * CH, :] = (wd_ref[...].astype(jnp.float32) * gain).astype(jnp.bfloat16)

    def weights(src_z):
        feats = pl.ds(pl.multiple_of(src_z * 2 * FEATS, 2 * FEATS), 2 * FEATS)
        wv_t = wv_ref[feats, :].astype(jnp.float32).T * gain_ref[:, feats]
        return jnp.concatenate([wv_t.astype(jnp.bfloat16), wt[:, feats]], axis=0)

    def compute(sub, sources, first):
        ws = [weights(src) for src in sources]

        @pl.loop(0, HALF // TILE)
        def _(i):
            lanes = pl.ds(pl.multiple_of(sub * HALF + i * TILE, TILE), TILE)
            total = None
            sq = None
            for src, w in zip(sources, ws):
                x = xt[pl.ds(pl.multiple_of(src * 2 * FEATS, 2 * FEATS), 2 * FEATS), lanes]
                term = jnp.dot(w, x, preferred_element_type=jnp.float32)
                total = term if total is None else total + term
                xf = x.astype(jnp.float32)
                part = jnp.sum((xf * xf).reshape(2 * FEATS // 8, 8, TILE), axis=0)
                sq = part if sq is None else sq + part
            if first:
                acc[:, lanes] = total
                squares[:, lanes] = sq
            else:
                acc[:, lanes] += total
                squares[:, lanes] += sq

    for sub in range(2):
        pair(z, sub, 0).wait_recv()
        compute(sub, [z], True)

    def above(s):
        return lax.rem(z + s, N_Z)

    def below(s):
        return lax.rem(z - s + 2 * N_Z, N_Z)

    @pl.loop(1, 8)
    def _(s):
        for sub in range(2):
            ring(0, sub, s).wait_recv()
            if sub == 0:
                ring(0, sub, s + 1).start()
            else:
                @pl.when(s < 7)
                def _():
                    ring(0, sub, s + 1).start()
            pair(below(s), sub, s).start()
            ring(1, sub, s).wait_recv()
            if sub == 1:
                ring(1, sub, s + 1).start()
            else:
                @pl.when(s < 7)
                def _():
                    ring(1, sub, s + 1).start()
            pair(above(s), sub, 8 + s).start()

            @pl.when(s > 1)
            def _():
                pair(below(s - 1), sub, s - 1).wait_recv()
                pair(above(s - 1), sub, 7 + s).wait_recv()
                compute(sub, [below(s - 1), above(s - 1)], False)

    for sub in range(2):
        ring(sub, sub, 8).wait_recv()
        pair(below(8), sub, 8).start()
        pair(below(7), sub, 7).wait_recv()
        pair(above(7), sub, 15).wait_recv()
        compute(sub, [below(7), above(7)], False)
    for sub in range(2):
        pair(below(8), sub, 8).wait_recv()
        compute(sub, [below(8)], False)

    inverse = lax.rsqrt(jnp.sum(squares[...], axis=0, keepdims=True) * (1.0 / MODEL) + EPS)
    key = (acc[VALS : VALS + CH, :] * inverse).astype(jnp.bfloat16).astype(jnp.float32)
    gate = (acc[VALS + CH : VALS + 2 * CH, :] * inverse).astype(jnp.bfloat16).astype(jnp.float32)

    @pl.loop(0, VALS // 64)
    def _(i):
        rows = pl.ds(pl.multiple_of(i * 64, 64), 64)
        vt_bf[rows, :] = (acc[rows, :] * inverse).astype(jnp.bfloat16)

    u = gate + column_of(bias_ref[...]) + drift_ref[...]
    log_decay = (jnp.minimum(u, 0.0) - jnp.log1p(jnp.exp(-jnp.abs(u)))) * (1.0 / GATE_NORM)
    blocks = SPAN // 128
    stacked = jnp.concatenate([log_decay[:, 128 * b : 128 * b + 128] for b in range(blocks)], axis=0)
    after = lax.broadcasted_iota(jnp.int32, (128, 128), 0) > lax.broadcasted_iota(jnp.int32, (128, 128), 1)
    local = jnp.dot(
        stacked, jnp.where(after, 1.0, 0.0), precision=lax.Precision.HIGHEST,
        preferred_element_type=jnp.float32,
    )
    sums = jnp.sum(stacked, axis=1, keepdims=True)
    run = jnp.zeros((CH, 1), jnp.float32)
    pieces = [None] * blocks
    for b in reversed(range(blocks)):
        rest = local[CH * b : CH * b + CH] + run
        pieces[b] = (key[:, 128 * b : 128 * b + 128] * jnp.exp(rest)).astype(jnp.bfloat16)
        run = run + sums[CH * b : CH * b + CH]
    weighted = jnp.concatenate(pieces, axis=1)
    partial = lax.dot_general(
        weighted, vt_bf[...], (((1,), (1,)), ((), ())), preferred_element_type=jnp.float32
    )

    group = lax.broadcasted_iota(jnp.int32, (8, 128), 1) // VT
    decay_tile = tile_of(run, group)
    for c in range(4):
        quarter = [partial[8 * a : 8 * a + 8, 128 * c : 128 * c + 128] for a in range(4)]
        for d in range(4):
            out = None
            for a in range(4):
                shift = (VT * (a - d)) % 128
                moved = quarter[a] if shift == 0 else pltpu.roll(quarter[a], shift, 1)
                out = moved if out is None else jnp.where(group == a, moved, out)
            msg[4 * c + d, 0:8, :] = out
            msg[4 * c + d, 8:16, :] = decay_tile

    def exchange(o):
        to = lax.rem(j + o, N_SP)
        return pltpu.make_async_remote_copy(
            src_ref=msg.at[to], dst_ref=got.at[j], send_sem=p_send.at[o], recv_sem=p_recv.at[o],
            device_id=(to, t), device_id_type=MESH,
        )

    @pl.loop(1, N_SP)
    def _(o):
        exchange(o).start()

    got[j] = msg[j]
    q_tile = tile_of(column_of(q_ref[...].astype(jnp.float32)) * KEY_CHANNELS ** (-0.5), group)

    @pl.loop(1, N_SP)
    def _(o):
        exchange(o).wait_recv()

    later = jnp.zeros((8, 128), jnp.float32)
    state = jnp.zeros((8, 128), jnp.float32)
    for i in reversed(range(N_SP)):
        state = state + jnp.exp(later) * got[i, 0:8, :]
        later = later + got[i, 8:16, :]
    read_msg[...] = jnp.sum(q_tile * state, axis=0, keepdims=True)

    def tell(o):
        return pltpu.make_async_remote_copy(
            src_ref=read_msg, dst_ref=read_got.at[t], send_sem=r_send.at[o], recv_sem=r_recv.at[o],
            device_id=(j, lax.rem(t + o, N_TP)), device_id_type=MESH,
        )

    @pl.loop(1, N_TP)
    def _(o):
        tell(o).start()

    read_got[t] = read_msg[...]
    state_ref[...] = jnp.concatenate([state[:, VT * a : VT * a + VT] for a in range(4)], axis=0).astype(jnp.bfloat16)

    @pl.loop(1, N_TP)
    def _(o):
        tell(o).wait_recv()

    lane_group = lax.broadcasted_iota(jnp.int32, (1, 128), 1) // VT
    reads = []
    sq = jnp.zeros((1, 128), jnp.float32)
    for h in range(HEADS):
        total = read_got[8 * h]
        for i in range(1, 8):
            total = total + read_got[8 * h + i]
        total = total + pltpu.roll(total, 64, 1)
        total = total + pltpu.roll(total, 32, 1)
        reads.append(total)
        own = jnp.sum(jnp.where(lane_group == 0, total * total, 0.0), axis=1, keepdims=True)
        sq = jnp.where(lane_group == h, jnp.broadcast_to(own, (1, 128)), sq)
    sq_msg[...] = sq

    def share(o):
        return pltpu.make_async_remote_copy(
            src_ref=sq_msg, dst_ref=sq_got.at[j], send_sem=s_send.at[o], recv_sem=s_recv.at[o],
            device_id=(lax.rem(j + o, N_SP), t), device_id_type=MESH,
        )

    @pl.loop(1, N_SP)
    def _(o):
        share(o).start()

    sq_got[j] = sq_msg[...]

    @pl.loop(1, N_SP)
    def _(o):
        share(o).wait_recv()

    whole = sq_got[0]
    for i in range(1, N_SP):
        whole = whole + sq_got[i]
    scale = lax.rsqrt(whole * (1.0 / VALS) + EPS)
    for h in range(HEADS):
        factor = scale[:, VT * h : VT * h + VT]
        read_ref[h : h + 1, :] = reads[h][:, 0:VT] * factor * og_ref[h : h + 1, :]

    @pl.loop(1, 8)
    def _(s):
        for sub in range(2):
            for way in range(2):
                ring(way, sub, s).wait_send()
            pair(below(s), sub, s).wait_send()
            pair(above(s), sub, 8 + s).wait_send()

    for sub in range(2):
        ring(sub, sub, 8).wait_send()
        pair(z, sub, 0).wait_send()
        pair(below(8), sub, 8).wait_send()

    @pl.loop(1, N_SP)
    def _(o):
        exchange(o).wait_send()
        share(o).wait_send()

    @pl.loop(1, N_TP)
    def _(o):
        tell(o).wait_send()


def body(tokens, norm_gain, w_key, w_decay, w_value, decay_bias, gate_drift, queries, out_gain):
    dma = pltpu.SemaphoreType.DMA
    vmem = pl.BlockSpec(memory_space=pltpu.VMEM)
    f32, bf16 = jnp.float32, jnp.bfloat16
    return pl.pallas_call(
        kernel,
        out_shape=(jax.ShapeDtypeStruct((CH, VT), bf16), jax.ShapeDtypeStruct((HEADS, VT), f32)),
        in_specs=[vmem] * 9,
        out_specs=(vmem, vmem),
        scratch_shapes=[
            pltpu.VMEM((MODEL, SPAN), bf16),
            pltpu.VMEM((2 * CH, MODEL), bf16),
            pltpu.VMEM((VALS + 2 * CH, SPAN), f32),
            pltpu.VMEM((8, SPAN), f32),
            pltpu.VMEM((VALS, SPAN), bf16),
            pltpu.VMEM((N_SP, 16, 128), f32),
            pltpu.VMEM((N_SP, 16, 128), f32),
            pltpu.VMEM((1, 128), f32),
            pltpu.VMEM((N_TP, 1, 128), f32),
            pltpu.VMEM((1, 128), f32),
            pltpu.VMEM((N_SP, 1, 128), f32),
            dma((2, 2, 9)), dma((2, 2, 9)), dma((16, 2)), dma((16, 2)),
            dma((N_SP,)), dma((N_SP,)), dma((N_TP,)), dma((N_TP,)), dma((N_SP,)), dma((N_SP,)),
        ],
        compiler_params=pltpu.CompilerParams(
            collective_id=0, has_side_effects=True, vmem_limit_bytes=50 * 1024 * 1024
        ),
    )(
        tokens.T, norm_gain.reshape(1, MODEL), w_key.T, w_decay.T, w_value, decay_bias.reshape(1, CH),
        gate_drift.reshape(1, SPAN), queries.reshape(1, CH), out_gain,
    )


def solution(mesh):
    return jax.shard_map(
        body,
        mesh=mesh,
        in_specs=(
            P("sp", "tp"), P(), P(None, "tp"), P(None, "tp"), P(), P("tp"), P("sp"), P("tp"), P(None, "sp"),
        ),
        out_specs=(P("tp", "sp"), P(None, "sp")),
        check_vma=False,
    )
```

```python
import functools

import jax
import jax.numpy as jnp
from jax import lax
from jax.experimental import pallas as pl
from jax.experimental.pallas import tpu as pltpu
from jax.sharding import PartitionSpec as P

MESH = pl.DeviceIdType.MESH
EPS = 1e-06
GATE_NORM = 16.0
KEY_CHANNELS = 256
N_SP, N_TP, N_Z = 16, 32, 16
SPAN, FEATS, VALS, CH = 2048, 64, 512, 32
SUBS = 4
SUB = SPAN // SUBS
VT = 32
HEADS = 4
MODEL = N_TP * FEATS


def column_of(row):
    n = row.shape[1]
    on_diagonal = lax.broadcasted_iota(jnp.int32, (n, n), 0) == lax.broadcasted_iota(jnp.int32, (n, n), 1)
    return jnp.sum(jnp.where(on_diagonal, jnp.broadcast_to(row, (n, n)), 0.0), axis=1, keepdims=True)


def tile_of(col, group):
    out = jnp.broadcast_to(col[0:8], (8, 128))
    for a in range(1, 4):
        out = jnp.where(group == a, jnp.broadcast_to(col[8 * a : 8 * a + 8], (8, 128)), out)
    return out


def kernel(
    x_hbm, gain_hbm, wk_hbm, wd_hbm, wv_hbm, bias_hbm, drift_hbm, q_hbm, og_hbm,
    state_ref, read_ref,
    xt, gain_ref, wk_ref, wd_ref, wv_ref, bias_ref, drift_ref, q_ref, og_ref,
    wt, acc, squares, msg, got, decay_msg, decay_got, read_msg, read_got, sq_msg, sq_got,
    in_sem, ring_send, ring_recv, pair_send, pair_recv,
    p_send, p_recv, d_send, d_recv, r_send, r_recv, s_send, s_recv,
):
    j = lax.axis_index("sp")
    t = lax.axis_index("tp")
    z, k = t // 2, t % 2
    sibling = 2 * z + 1 - k
    up = 2 * lax.rem(z + 1, N_Z) + k
    down = 2 * lax.rem(z + N_Z - 1, N_Z) + k

    barrier = pltpu.get_barrier_semaphore()
    for other in (sibling, up, down):
        pl.semaphore_signal(barrier, inc=1, device_id=(j, other), device_id_type=MESH)

    @pl.loop(1, N_SP)
    def _(o):
        pl.semaphore_signal(barrier, inc=1, device_id=(lax.rem(j + o, N_SP), t), device_id_type=MESH)

    def rows_of(src_z, core):
        return pl.ds(pl.multiple_of((2 * src_z + core) * FEATS, FEATS), FEATS)

    def lanes_of(sub):
        return pl.ds(sub * SUB, SUB)

    loads = [
        pltpu.make_async_copy(src, dst, in_sem.at[i])
        for i, (src, dst) in enumerate(
            [
                (x_hbm, xt.at[rows_of(z, k), :]), (gain_hbm, gain_ref), (wk_hbm, wk_ref), (wd_hbm, wd_ref),
                (wv_hbm, wv_ref), (bias_hbm, bias_ref), (drift_hbm, drift_ref), (q_hbm, q_ref), (og_hbm, og_ref),
            ]
        )
    ]
    for load in loads:
        load.start()

    def ring(way, sub, s):
        src_z = lax.rem(z - (s - 1) + 2 * N_Z, N_Z) if way == 0 else lax.rem(z + (s - 1), N_Z)
        place = xt.at[rows_of(src_z, k), lanes_of(sub)]
        return pltpu.make_async_remote_copy(
            src_ref=place, dst_ref=place,
            send_sem=ring_send.at[way, sub, s], recv_sem=ring_recv.at[way, sub, s],
            device_id=(j, up if way == 0 else down), device_id_type=MESH,
        )

    def pair(src_z, sub, slot):
        place = xt.at[rows_of(src_z, k), lanes_of(sub)]
        return pltpu.make_async_remote_copy(
            src_ref=place, dst_ref=place,
            send_sem=pair_send.at[slot, sub], recv_sem=pair_recv.at[slot, sub],
            device_id=(j, sibling), device_id_type=MESH,
        )

    def above(s):
        return lax.rem(z + s, N_Z)

    def below(s):
        return lax.rem(z - s + 2 * N_Z, N_Z)

    def long_way(sub):
        return 0 if sub >= SUBS // 2 else 1

    order = list(reversed(range(SUBS)))

    loads[0].wait()
    pl.semaphore_wait(barrier, 3 + N_SP - 1)
    for sub in order:
        for way in range(2):
            ring(way, sub, 1).start()
    for sub in order:
        pair(z, sub, 0).start()
    for load in loads[1:]:
        load.wait()

    gain = gain_ref[...]
    wt[VALS : VALS + CH, :] = (wk_ref[...].astype(jnp.float32) * gain).astype(jnp.bfloat16)
    wt[VALS + CH : VALS + 2 * CH, :] = (wd_ref[...].astype(jnp.float32) * gain).astype(jnp.bfloat16)

    def feats_of(src_z):
        return pl.ds(pl.multiple_of(src_z * 2 * FEATS, 2 * FEATS), 2 * FEATS)

    def prepare(src_z):
        feats = feats_of(src_z)
        wt[0:VALS, feats] = (wv_ref[feats, :].astype(jnp.float32).T * gain_ref[:, feats]).astype(jnp.bfloat16)

    def compute(sub, sources, first=False):
        lanes = lanes_of(sub)
        total = None
        sq = None
        for src in sources:
            x = xt[feats_of(src), lanes]
            term = jnp.dot(wt[:, feats_of(src)], x, preferred_element_type=jnp.float32)
            total = term if total is None else total + term
            xf = x.astype(jnp.float32)
            part = jnp.sum((xf * xf).reshape(2 * FEATS // 8, 8, SUB), axis=0)
            sq = part if sq is None else sq + part
        if first:
            acc[:, lanes] = total
            squares[:, lanes] = sq
        else:
            acc[:, lanes] += total
            squares[:, lanes] += sq

    prepare(z)

    @pl.loop(1, 8)
    def _(s):
        for at, sub in enumerate(order):
            long = long_way(sub)
            ring(long, sub, s).wait_recv()
            ring(long, sub, s + 1).start()
            pair(below(s) if long == 0 else above(s), sub, s + 8 * long).start()
            ring(1 - long, sub, s).wait_recv()

            @pl.when(s < 7)
            def _():
                ring(1 - long, sub, s + 1).start()

            pair(above(s) if long == 0 else below(s), sub, s + 8 * (1 - long)).start()
            if at == 0:
                prepare(below(s))
            if at == 1:
                prepare(above(s))

            @pl.when(s > 1)
            def _():
                pair(below(s - 1), sub, s - 1).wait_recv()
                pair(above(s - 1), sub, 7 + s).wait_recv()
                compute(sub, [below(s - 1), above(s - 1)])

            @pl.when(s == 1)
            def _():
                pair(z, sub, 0).wait_recv()
                compute(sub, [z], True)

    prepare(below(8))
    for sub in order:
        pair(below(7), sub, 7).wait_recv()
        pair(above(7), sub, 15).wait_recv()
        compute(sub, [below(7), above(7)])
        ring(long_way(sub), sub, 8).wait_recv()
        pair(below(8), sub, 8).start()

    group = lax.broadcasted_iota(jnp.int32, (8, 128), 1) // VT
    bias = column_of(bias_ref[...])
    q_tile = tile_of(column_of(q_ref[...].astype(jnp.float32)) * KEY_CHANNELS ** (-0.5), group)
    after = lax.broadcasted_iota(jnp.int32, (128, 128), 0) > lax.broadcasted_iota(jnp.int32, (128, 128), 1)
    after = jnp.where(after, 1.0, 0.0)

    def to_sp(o, source, target, send, recv):
        to = lax.rem(j + o, N_SP)
        return pltpu.make_async_remote_copy(
            src_ref=source if len(source.shape) == 2 else source.at[to], dst_ref=target.at[j],
            send_sem=send.at[o], recv_sem=recv.at[o], device_id=(to, t), device_id_type=MESH,
        )

    def decays(o):
        return to_sp(o, decay_msg, decay_got, d_send, d_recv)

    def exchange(o):
        return to_sp(o, msg, got, p_send, p_recv)

    run = jnp.zeros((CH, 1), jnp.float32)
    partial = jnp.zeros((CH, VALS), jnp.float32)
    blocks = SUB // 128
    for sub in order:
        lanes = lanes_of(sub)
        pair(below(8), sub, 8).wait_recv()
        compute(sub, [below(8)])
        inverse = lax.rsqrt(jnp.sum(squares[:, lanes], axis=0, keepdims=True) * (1.0 / MODEL) + EPS)
        gate = (acc[VALS + CH : VALS + 2 * CH, lanes] * inverse).astype(jnp.bfloat16).astype(jnp.float32)
        key = (acc[VALS : VALS + CH, lanes] * inverse).astype(jnp.bfloat16).astype(jnp.float32)
        u = gate + bias + drift_ref[:, lanes]
        log_decay = (jnp.minimum(u, 0.0) - jnp.log1p(jnp.exp(-jnp.abs(u)))) * (1.0 / GATE_NORM)
        stacked = jnp.concatenate([log_decay[:, 128 * b : 128 * b + 128] for b in range(blocks)], axis=0)
        local = jnp.dot(stacked, after, precision=lax.Precision.HIGHEST, preferred_element_type=jnp.float32)
        sums = jnp.sum(stacked, axis=1, keepdims=True)
        pieces = [None] * blocks
        for b in reversed(range(blocks)):
            rest = local[CH * b : CH * b + CH] + run
            pieces[b] = (key[:, 128 * b : 128 * b + 128] * jnp.exp(rest)).astype(jnp.bfloat16)
            run = run + sums[CH * b : CH * b + CH]
        if sub == 0:
            decay_msg[...] = tile_of(run, group)

            @pl.loop(1, N_SP)
            def _(o):
                decays(o).start()

        weighted = jnp.concatenate(pieces, axis=1)
        value = (acc[0:VALS, lanes] * inverse).astype(jnp.bfloat16)
        partial = partial + lax.dot_general(
            weighted, value, (((1,), (1,)), ((), ())), preferred_element_type=jnp.float32
        )

    for c in range(4):
        quarter = [partial[8 * a : 8 * a + 8, 128 * c : 128 * c + 128] for a in range(4)]
        for d in range(4):
            out = None
            for a in range(4):
                shift = (VT * (a - d)) % 128
                moved = quarter[a] if shift == 0 else pltpu.roll(quarter[a], shift, 1)
                out = moved if out is None else jnp.where(group == a, moved, out)
            msg[4 * c + d] = out

    @pl.loop(1, N_SP)
    def _(o):
        exchange(o).start()

    got[j] = msg[j]
    decay_got[j] = decay_msg[...]

    @pl.loop(1, N_SP)
    def _(o):
        decays(o).wait_recv()

    later = jnp.zeros((8, 128), jnp.float32)
    factors = [None] * N_SP
    for i in reversed(range(N_SP)):
        factors[i] = jnp.exp(later)
        later = later + decay_got[i]

    @pl.loop(1, N_SP)
    def _(o):
        exchange(o).wait_recv()

    state = factors[0] * got[0]
    for i in range(1, N_SP):
        state = state + factors[i] * got[i]
    read_msg[...] = jnp.sum(q_tile * state, axis=0, keepdims=True)

    def tell(o):
        return pltpu.make_async_remote_copy(
            src_ref=read_msg, dst_ref=read_got.at[t], send_sem=r_send.at[o], recv_sem=r_recv.at[o],
            device_id=(j, lax.rem(t + o, N_TP)), device_id_type=MESH,
        )

    @pl.loop(0, N_TP - 1)
    def _(i):
        tell(lax.rem(i + N_TP // 2 - 1, N_TP - 1) + 1).start()

    read_got[t] = read_msg[...]
    state_ref[...] = jnp.concatenate([state[:, VT * a : VT * a + VT] for a in range(4)], axis=0).astype(jnp.bfloat16)

    @pl.loop(1, 8)
    def _(s):
        for sub in range(SUBS):
            for way in range(2):
                ring(way, sub, s).wait_send()
            pair(below(s), sub, s).wait_send()
            pair(above(s), sub, 8 + s).wait_send()

    for sub in range(SUBS):
        ring(long_way(sub), sub, 8).wait_send()
        pair(z, sub, 0).wait_send()
        pair(below(8), sub, 8).wait_send()

    @pl.loop(1, N_SP)
    def _(o):
        exchange(o).wait_send()
        decays(o).wait_send()

    @pl.loop(1, N_TP)
    def _(o):
        tell(o).wait_recv()

    lane_group = lax.broadcasted_iota(jnp.int32, (1, 128), 1) // VT
    reads = []
    sq = jnp.zeros((1, 128), jnp.float32)
    for h in range(HEADS):
        total = read_got[8 * h]
        for i in range(1, 8):
            total = total + read_got[8 * h + i]
        total = total + pltpu.roll(total, 64, 1)
        total = total + pltpu.roll(total, 32, 1)
        reads.append(total)
        own = jnp.sum(jnp.where(lane_group == 0, total * total, 0.0), axis=1, keepdims=True)
        sq = jnp.where(lane_group == h, jnp.broadcast_to(own, (1, 128)), sq)
    sq_msg[...] = sq

    def share(o):
        return to_sp(o, sq_msg, sq_got, s_send, s_recv)

    @pl.loop(1, N_SP)
    def _(o):
        share(o).start()

    sq_got[j] = sq_msg[...]

    @pl.loop(1, N_TP)
    def _(o):
        tell(o).wait_send()

    @pl.loop(1, N_SP)
    def _(o):
        share(o).wait_recv()

    whole = sq_got[0]
    for i in range(1, N_SP):
        whole = whole + sq_got[i]
    scale = lax.rsqrt(whole * (1.0 / VALS) + EPS)
    for h in range(HEADS):
        factor = scale[:, VT * h : VT * h + VT]
        read_ref[h : h + 1, :] = reads[h][:, 0:VT] * factor * og_ref[h : h + 1, :]

    @pl.loop(1, N_SP)
    def _(o):
        share(o).wait_send()


def body(tokens, norm_gain, w_key, w_decay, w_value, decay_bias, gate_drift, queries, out_gain):
    dma = pltpu.SemaphoreType.DMA
    vmem = pl.BlockSpec(memory_space=pltpu.VMEM)
    f32, bf16 = jnp.float32, jnp.bfloat16
    return pl.pallas_call(
        kernel,
        out_shape=(jax.ShapeDtypeStruct((CH, VT), bf16), jax.ShapeDtypeStruct((HEADS, VT), f32)),
        in_specs=[pl.BlockSpec(memory_space=pl.ANY)] * 9,
        out_specs=(vmem, vmem),
        scratch_shapes=[
            pltpu.VMEM((MODEL, SPAN), bf16),
            pltpu.VMEM((1, MODEL), f32),
            pltpu.VMEM((CH, MODEL), bf16),
            pltpu.VMEM((CH, MODEL), bf16),
            pltpu.VMEM((MODEL, VALS), bf16),
            pltpu.VMEM((1, CH), f32),
            pltpu.VMEM((1, SPAN), f32),
            pltpu.VMEM((1, CH), bf16),
            pltpu.VMEM((HEADS, VT), f32),
            pltpu.VMEM((VALS + 2 * CH, MODEL), bf16),
            pltpu.VMEM((VALS + 2 * CH, SPAN), f32),
            pltpu.VMEM((8, SPAN), f32),
            pltpu.VMEM((N_SP, 8, 128), f32),
            pltpu.VMEM((N_SP, 8, 128), f32),
            pltpu.VMEM((8, 128), f32),
            pltpu.VMEM((N_SP, 8, 128), f32),
            pltpu.VMEM((1, 128), f32),
            pltpu.VMEM((N_TP, 1, 128), f32),
            pltpu.VMEM((1, 128), f32),
            pltpu.VMEM((N_SP, 1, 128), f32),
            dma((9,)), dma((2, SUBS, 9)), dma((2, SUBS, 9)), dma((16, SUBS)), dma((16, SUBS)),
            dma((N_SP,)), dma((N_SP,)), dma((N_SP,)), dma((N_SP,)), dma((N_TP,)), dma((N_TP,)), dma((N_SP,)), dma((N_SP,)),
        ],
        compiler_params=pltpu.CompilerParams(
            collective_id=0, has_side_effects=True, vmem_limit_bytes=67043328
        ),
    )(
        tokens.T, norm_gain.reshape(1, MODEL), w_key.T, w_decay.T, w_value, decay_bias.reshape(1, CH),
        gate_drift.reshape(1, SPAN), queries.reshape(1, CH), out_gain,
    )


def solution(mesh):
    return jax.shard_map(
        body,
        mesh=mesh,
        in_specs=(
            P("sp", "tp"), P(), P(None, "tp"), P(None, "tp"), P(), P("tp"), P("sp"), P("tp"), P(None, "sp"),
        ),
        out_specs=(P("tp", "sp"), P(None, "sp")),
        check_vma=False,
    )
```

```python
import functools

import jax
import jax.numpy as jnp
from jax import lax
from jax.experimental import pallas as pl
from jax.experimental.pallas import tpu as pltpu
from jax.sharding import PartitionSpec as P

MESH = pl.DeviceIdType.MESH
EPS = 1e-06
GATE_NORM = 16.0
KEY_CHANNELS = 256
N_SP, N_TP, N_Z = 16, 32, 16
SPAN, FEATS, VALS, CH = 2048, 64, 512, 32
SUBS = 4
SUB = SPAN // SUBS
VT = 32
HEADS = 4
MODEL = N_TP * FEATS


def hops(step, size):
    return min(step, size - step)


SP_ORDER = sorted(range(1, N_SP), key=lambda o: -(hops(o // 4, 4) + hops(o % 4, 4)))
TP_ORDER = sorted(range(1, N_TP), key=lambda o: -hops(o // 2, N_Z))


def column_of(row):
    n = row.shape[1]
    on_diagonal = lax.broadcasted_iota(jnp.int32, (n, n), 0) == lax.broadcasted_iota(jnp.int32, (n, n), 1)
    return jnp.sum(jnp.where(on_diagonal, jnp.broadcast_to(row, (n, n)), 0.0), axis=1, keepdims=True)


def tile_of(col, group):
    out = jnp.broadcast_to(col[0:8], (8, 128))
    for a in range(1, 4):
        out = jnp.where(group == a, jnp.broadcast_to(col[8 * a : 8 * a + 8], (8, 128)), out)
    return out


def kernel(
    x_hbm, gain_hbm, wk_hbm, wd_hbm, wv_hbm, bias_hbm, drift_hbm, q_hbm, og_hbm,
    out_ref,
    xt, gain_ref, wk_ref, wd_ref, wv_ref, bias_ref, drift_ref, q_ref, og_ref,
    wt, acc, squares, msg, got, decay_msg, decay_got, read_msg, read_got, sq_msg, sq_got,
    near_sem, in_sem, ring_send, ring_recv, pair_send, pair_recv,
    p_send, p_recv, d_send, d_recv, r_send, r_recv, s_send, s_recv,
):
    j = lax.axis_index("sp")
    t = lax.axis_index("tp")
    z, k = t // 2, t % 2
    sibling = 2 * z + 1 - k
    up = 2 * lax.rem(z + 1, N_Z) + k
    down = 2 * lax.rem(z + N_Z - 1, N_Z) + k

    barrier = pltpu.get_barrier_semaphore()
    for other in (sibling, up, down):
        pl.semaphore_signal(barrier, inc=1, device_id=(j, other), device_id_type=MESH)
    y, x = j // 4, j % 4

    def at_sp(dy, dx):
        return lax.rem(y + dy, 4) * 4 + lax.rem(x + dx, 4)

    beside = (at_sp(0, 1), at_sp(0, 3))
    across = (at_sp(1, 0), at_sp(3, 0))
    for other in beside + across:
        pl.semaphore_signal(barrier, inc=1, device_id=(other, t), device_id_type=MESH)

    def rows_of(src_z, core):
        return pl.ds(pl.multiple_of((2 * src_z + core) * FEATS, FEATS), FEATS)

    def lanes_of(sub):
        return pl.ds(sub * SUB, SUB)

    loads = [
        pltpu.make_async_copy(src, dst, in_sem.at[i])
        for i, (src, dst) in enumerate(
            [
                (x_hbm, xt.at[rows_of(z, k), :]), (gain_hbm, gain_ref), (wk_hbm, wk_ref), (wd_hbm, wd_ref),
                (wv_hbm, wv_ref), (bias_hbm, bias_ref), (drift_hbm, drift_ref), (q_hbm, q_ref), (og_hbm, og_ref),
            ]
        )
    ]
    for load in loads:
        load.start()

    def ring(way, sub, s):
        src_z = lax.rem(z - (s - 1) + 2 * N_Z, N_Z) if way == 0 else lax.rem(z + (s - 1), N_Z)
        place = xt.at[rows_of(src_z, k), lanes_of(sub)]
        return pltpu.make_async_remote_copy(
            src_ref=place, dst_ref=place,
            send_sem=ring_send.at[way, sub, s], recv_sem=ring_recv.at[way, sub, s],
            device_id=(j, up if way == 0 else down), device_id_type=MESH,
        )

    def pair(src_z, sub, slot):
        place = xt.at[rows_of(src_z, k), lanes_of(sub)]
        return pltpu.make_async_remote_copy(
            src_ref=place, dst_ref=place,
            send_sem=pair_send.at[slot, sub], recv_sem=pair_recv.at[slot, sub],
            device_id=(j, sibling), device_id_type=MESH,
        )

    def above(s):
        return lax.rem(z + s, N_Z)

    def below(s):
        return lax.rem(z - s + 2 * N_Z, N_Z)

    def long_way(sub):
        return 0 if sub >= SUBS // 2 else 1

    order = list(reversed(range(SUBS)))

    loads[0].wait()
    pl.semaphore_wait(barrier, 7)
    for sub in order:
        for way in range(2):
            ring(way, sub, 1).start()
    for sub in order:
        pair(z, sub, 0).start()

    def pass_on(phase, others):
        for other in others:
            pl.semaphore_signal(near_sem.at[phase], inc=1, device_id=(other, t), device_id_type=MESH)

    pass_on(0, beside)
    for load in loads[1:]:
        load.wait()

    gain = gain_ref[...]
    wt[VALS : VALS + CH, :] = (wk_ref[...].astype(jnp.float32) * gain).astype(jnp.bfloat16)
    wt[VALS + CH : VALS + 2 * CH, :] = (wd_ref[...].astype(jnp.float32) * gain).astype(jnp.bfloat16)

    def feats_of(src_z):
        return pl.ds(pl.multiple_of(src_z * 2 * FEATS, 2 * FEATS), 2 * FEATS)

    def prepare(src_z):
        feats = feats_of(src_z)
        wt[0:VALS, feats] = (wv_ref[feats, :].astype(jnp.float32).T * gain_ref[:, feats]).astype(jnp.bfloat16)

    def compute(sub, sources, first=False):
        lanes = lanes_of(sub)
        total = None
        sq = None
        for src in sources:
            x = xt[feats_of(src), lanes]
            term = jnp.dot(wt[:, feats_of(src)], x, preferred_element_type=jnp.float32)
            total = term if total is None else total + term
            xf = x.astype(jnp.float32)
            part = jnp.sum((xf * xf).reshape(2 * FEATS // 8, 8, SUB), axis=0)
            sq = part if sq is None else sq + part
        if first:
            acc[:, lanes] = total
            squares[:, lanes] = sq
        else:
            acc[:, lanes] += total
            squares[:, lanes] += sq

    prepare(z)

    @pl.loop(1, 8)
    def _(s):
        for at, sub in enumerate(order):
            long = long_way(sub)
            ring(long, sub, s).wait_recv()
            ring(long, sub, s + 1).start()
            pair(below(s) if long == 0 else above(s), sub, s + 8 * long).start()
            ring(1 - long, sub, s).wait_recv()

            @pl.when(s < 7)
            def _():
                ring(1 - long, sub, s + 1).start()

            pair(above(s) if long == 0 else below(s), sub, s + 8 * (1 - long)).start()
            if at == 0:
                prepare(below(s))
            if at == 1:
                prepare(above(s))

            @pl.when(s > 1)
            def _():
                pair(below(s - 1), sub, s - 1).wait_recv()
                pair(above(s - 1), sub, 7 + s).wait_recv()
                compute(sub, [below(s - 1), above(s - 1)])

            @pl.when(s == 1)
            def _():
                pair(z, sub, 0).wait_recv()
                compute(sub, [z], True)

        for phase in range(3):
            @pl.when(s == phase + 2)
            def _():
                pl.semaphore_wait(near_sem.at[phase], 2)
                if phase < 2:
                    pass_on(phase + 1, across)

    prepare(below(8))
    for sub in order:
        pair(below(7), sub, 7).wait_recv()
        pair(above(7), sub, 15).wait_recv()
        compute(sub, [below(7), above(7)])
        ring(long_way(sub), sub, 8).wait_recv()
        pair(below(8), sub, 8).start()

    group = lax.broadcasted_iota(jnp.int32, (8, 128), 1) // VT
    bias = column_of(bias_ref[...])
    q_tile = tile_of(column_of(q_ref[...].astype(jnp.float32)) * KEY_CHANNELS ** (-0.5), group)
    row_at = lax.broadcasted_iota(jnp.int32, (128, 256), 0)
    col_at = lax.broadcasted_iota(jnp.int32, (128, 256), 1)
    summing = jnp.where((row_at > col_at) | (col_at >= 128), 1.0, 0.0).astype(jnp.bfloat16)

    def to_sp(o, source, target, send, recv):
        to = at_sp(o // 4, o % 4)
        return pltpu.make_async_remote_copy(
            src_ref=source if len(source.shape) == 2 else source.at[to], dst_ref=target.at[j],
            send_sem=send.at[o], recv_sem=recv.at[o], device_id=(to, t), device_id_type=MESH,
        )

    def decays(o):
        return to_sp(o, decay_msg, decay_got, d_send, d_recv)

    def exchange(o):
        return to_sp(o, msg, got, p_send, p_recv)

    run = jnp.zeros((CH, 128), jnp.float32)
    partial = jnp.zeros((CH, VALS), jnp.float32)
    blocks = SUB // 128
    for sub in order:
        lanes = lanes_of(sub)
        pair(below(8), sub, 8).wait_recv()
        last = xt[feats_of(below(8)), lanes]
        last_w = wt[:, feats_of(below(8))]
        last_f = last.astype(jnp.float32)
        sq = squares[:, lanes] + jnp.sum((last_f * last_f).reshape(2 * FEATS // 8, 8, SUB), axis=0)
        inverse = lax.rsqrt(jnp.sum(sq, axis=0, keepdims=True) * (1.0 / MODEL) + EPS)
        both = acc[VALS : VALS + 2 * CH, lanes] + jnp.dot(last_w[VALS:], last, preferred_element_type=jnp.float32)
        both = (both * inverse).astype(jnp.bfloat16).astype(jnp.float32)
        key, gate = both[:CH], both[CH:]
        u = gate + bias + drift_ref[:, lanes]
        log_decay = (jnp.minimum(u, 0.0) - jnp.log1p(jnp.exp(-jnp.abs(u)))) * (1.0 / GATE_NORM)
        stacked = jnp.concatenate([log_decay[:, 128 * b : 128 * b + 128] for b in range(blocks)], axis=0)
        high = stacked.astype(jnp.bfloat16)
        left = stacked - high.astype(jnp.float32)
        mid = left.astype(jnp.bfloat16)
        low = (left - mid.astype(jnp.float32)).astype(jnp.bfloat16)
        summed = (
            jnp.dot(low, summing, preferred_element_type=jnp.float32)
            + jnp.dot(mid, summing, preferred_element_type=jnp.float32)
            + jnp.dot(high, summing, preferred_element_type=jnp.float32)
        )
        pieces = [None] * blocks
        for b in reversed(range(blocks)):
            rest = summed[CH * b : CH * b + CH, 0:128] + run
            pieces[b] = (key[:, 128 * b : 128 * b + 128] * jnp.exp(rest)).astype(jnp.bfloat16)
            run = run + summed[CH * b : CH * b + CH, 128:256]
        if sub == 0:
            decay_msg[...] = tile_of(run, group)
            for o in SP_ORDER:
                decays(o).start()

        weighted = jnp.concatenate(pieces, axis=1)
        value = acc[0:VALS, lanes] + jnp.dot(last_w[:VALS], last, preferred_element_type=jnp.float32)
        value = (value * inverse).astype(jnp.bfloat16)
        partial = partial + lax.dot_general(
            weighted, value, (((1,), (1,)), ((), ())), preferred_element_type=jnp.float32
        )

    for c in range(4):
        quarter = [partial[8 * a : 8 * a + 8, 128 * c : 128 * c + 128] for a in range(4)]
        for d in range(4):
            out = None
            for a in range(4):
                shift = (VT * (a - d)) % 128
                moved = quarter[a] if shift == 0 else pltpu.roll(quarter[a], shift, 1)
                out = moved if out is None else jnp.where(group == a, moved, out)
            msg[4 * c + d] = out

    for o in SP_ORDER:
        exchange(o).start()

    got[j] = msg[j]
    decay_got[j] = decay_msg[...]

    for o in SP_ORDER:
        decays(o).wait_recv()

    later = jnp.zeros((8, 128), jnp.float32)
    factors = [None] * N_SP
    for i in reversed(range(N_SP)):
        factors[i] = jnp.exp(later)
        later = later + decay_got[i]

    for o in SP_ORDER:
        exchange(o).wait_recv()

    state = factors[0] * got[0]
    for i in range(1, N_SP):
        state = state + factors[i] * got[i]
    read_msg[...] = jnp.sum(q_tile * state, axis=0, keepdims=True)

    def tell(o):
        return pltpu.make_async_remote_copy(
            src_ref=read_msg, dst_ref=read_got.at[t], send_sem=r_send.at[o], recv_sem=r_recv.at[o],
            device_id=(j, 2 * lax.rem(z + o // 2, N_Z) + lax.rem(k + o % 2, 2)), device_id_type=MESH,
        )

    for o in TP_ORDER:
        tell(o).start()

    read_got[t] = read_msg[...]
    out_ref[0:8, :] = state

    @pl.loop(1, 8)
    def _(s):
        for sub in range(SUBS):
            for way in range(2):
                ring(way, sub, s).wait_send()
            pair(below(s), sub, s).wait_send()
            pair(above(s), sub, 8 + s).wait_send()

    for sub in range(SUBS):
        ring(long_way(sub), sub, 8).wait_send()
        pair(z, sub, 0).wait_send()
        pair(below(8), sub, 8).wait_send()

    for o in SP_ORDER:
        exchange(o).wait_send()
        decays(o).wait_send()

    for o in TP_ORDER:
        tell(o).wait_recv()

    lane_group = lax.broadcasted_iota(jnp.int32, (1, 128), 1) // VT
    reads = []
    sq = jnp.zeros((1, 128), jnp.float32)
    for h in range(HEADS):
        total = read_got[8 * h]
        for i in range(1, 8):
            total = total + read_got[8 * h + i]
        total = total + pltpu.roll(total, 64, 1)
        total = total + pltpu.roll(total, 32, 1)
        reads.append(total)
        own = jnp.sum(jnp.where(lane_group == 0, total * total, 0.0), axis=1, keepdims=True)
        sq = jnp.where(lane_group == h, jnp.broadcast_to(own, (1, 128)), sq)
    sq_msg[...] = sq

    def share(o):
        return to_sp(o, sq_msg, sq_got, s_send, s_recv)

    for o in SP_ORDER:
        share(o).start()

    sq_got[j] = sq_msg[...]

    for o in TP_ORDER:
        tell(o).wait_send()

    for o in SP_ORDER:
        share(o).wait_recv()

    whole = sq_got[0]
    for i in range(1, N_SP):
        whole = whole + sq_got[i]
    scale = lax.rsqrt(whole * (1.0 / VALS) + EPS)
    for h in range(HEADS):
        factor = scale[:, VT * h : VT * h + VT]
        out_ref[8 + h : 9 + h, 0:VT] = reads[h][:, 0:VT] * factor * og_ref[h : h + 1, :]

    for o in SP_ORDER:
        share(o).wait_send()


def unpack(packed_ref, state_ref, read_ref):
    state = packed_ref[0:8, :]
    state_ref[...] = jnp.concatenate([state[:, VT * a : VT * a + VT] for a in range(4)], axis=0).astype(jnp.bfloat16)
    read_ref[...] = packed_ref[8 : 8 + HEADS, 0:VT]


def body(tokens, norm_gain, w_key, w_decay, w_value, decay_bias, gate_drift, queries, out_gain):
    dma = pltpu.SemaphoreType.DMA
    vmem = pl.BlockSpec(memory_space=pltpu.VMEM)
    f32, bf16 = jnp.float32, jnp.bfloat16
    packed = pl.pallas_call(
        kernel,
        out_shape=jax.ShapeDtypeStruct((16, 128), f32),
        in_specs=[pl.BlockSpec(memory_space=pl.ANY)] * 9,
        out_specs=vmem,
        scratch_shapes=[
            pltpu.VMEM((MODEL, SPAN), bf16),
            pltpu.VMEM((1, MODEL), f32),
            pltpu.VMEM((CH, MODEL), bf16),
            pltpu.VMEM((CH, MODEL), bf16),
            pltpu.VMEM((MODEL, VALS), bf16),
            pltpu.VMEM((1, CH), f32),
            pltpu.VMEM((1, SPAN), f32),
            pltpu.VMEM((1, CH), bf16),
            pltpu.VMEM((HEADS, VT), f32),
            pltpu.VMEM((VALS + 2 * CH, MODEL), bf16),
            pltpu.VMEM((VALS + 2 * CH, SPAN), f32),
            pltpu.VMEM((8, SPAN), f32),
            pltpu.VMEM((N_SP, 8, 128), f32),
            pltpu.VMEM((N_SP, 8, 128), f32),
            pltpu.VMEM((8, 128), f32),
            pltpu.VMEM((N_SP, 8, 128), f32),
            pltpu.VMEM((1, 128), f32),
            pltpu.VMEM((N_TP, 1, 128), f32),
            pltpu.VMEM((1, 128), f32),
            pltpu.VMEM((N_SP, 1, 128), f32),
            pltpu.SemaphoreType.REGULAR((3,)), dma((9,)), dma((2, SUBS, 9)), dma((2, SUBS, 9)), dma((16, SUBS)), dma((16, SUBS)),
            dma((N_SP,)), dma((N_SP,)), dma((N_SP,)), dma((N_SP,)), dma((N_TP,)), dma((N_TP,)), dma((N_SP,)), dma((N_SP,)),
        ],
        compiler_params=pltpu.CompilerParams(
            collective_id=0, has_side_effects=True, vmem_limit_bytes=67043328
        ),
    )(
        tokens.T, norm_gain.reshape(1, MODEL), w_key.T, w_decay.T, w_value, decay_bias.reshape(1, CH),
        gate_drift.reshape(1, SPAN), queries.reshape(1, CH), out_gain,
    )
    return pl.pallas_call(
        unpack,
        out_shape=(jax.ShapeDtypeStruct((CH, VT), bf16), jax.ShapeDtypeStruct((HEADS, VT), f32)),
        in_specs=[vmem],
        out_specs=(vmem, vmem),
    )(packed)


def solution(mesh):
    return jax.shard_map(
        body,
        mesh=mesh,
        in_specs=(
            P("sp", "tp"), P(), P(None, "tp"), P(None, "tp"), P(), P("tp"), P("sp"), P("tp"), P(None, "sp"),
        ),
        out_specs=(P("tp", "sp"), P(None, "sp")),
        check_vma=False,
    )
```

```python
import jax
import jax.numpy as jnp
from jax import lax
from jax.experimental import pallas as pl
from jax.experimental.pallas import tpu as pltpu
from jax.sharding import PartitionSpec as P

MESH = pl.DeviceIdType.MESH
EPS = 1e-06
GATE_NORM = 16.0
KEY_CHANNELS = 256
N_SP, N_TP, N_Z = 16, 32, 16
SPAN, FEATS, VALS, CH = 2048, 64, 512, 32
QUARTERS = 4
ROWS = SPAN // QUARTERS
NCH = QUARTERS * CH
VT = 32
HEADS = 4
MODEL = N_TP * FEATS
STEPS = 9
HIGH = lax.Precision.HIGHEST


def hops(step, size):
    return min(step, size - step)


def sp_hops(o):
    return hops(o // 4, 4) + hops(o % 4, 4)


SP_ORDER = sorted(range(1, N_SP), key=lambda o: -sp_hops(o))
TP_ORDER = sorted(range(1, N_TP), key=lambda o: -hops(o // 2, N_Z))
ALL_ORDER = sorted(range(1, 4 * N_SP), key=lambda o: -(hops(4 * (o // 16), N_Z) + sp_hops(o % 16)))


def column_of(row):
    n = row.shape[1]
    on_diagonal = lax.broadcasted_iota(jnp.int32, (n, n), 0) == lax.broadcasted_iota(jnp.int32, (n, n), 1)
    return jnp.sum(jnp.where(on_diagonal, jnp.broadcast_to(row, (n, n)), 0.0), axis=1, keepdims=True)


def lane_row(rows):
    at = lax.broadcasted_iota(jnp.int32, (VT, 128), 1)
    pick = jnp.where(lax.rem(at, VT) == lax.broadcasted_iota(jnp.int32, (VT, 128), 0), 1.0, 0.0)
    wide = jnp.dot(rows, pick, precision=HIGH, preferred_element_type=jnp.float32)
    lane = lax.broadcasted_iota(jnp.int32, (8, 128), 1) // VT
    mine = lane == lax.broadcasted_iota(jnp.int32, (8, 128), 0)
    return jnp.sum(jnp.where(mine, wide, 0.0), axis=0, keepdims=True)


def kernel(
    x_hbm, gain_hbm, wk_hbm, wd_hbm, wv_hbm, bias_hbm, drift_hbm, q_hbm, og_hbm,
    out_ref,
    xs, xt, gain_ref, wk_ref, wd_ref, wv_ref, bias_ref, drift_ref, q_ref, og_ref,
    wrel, acc, squares, small_msg, small_got, key_scr, gate_scr, msg, got, d_msg, d_got,
    read_msg, read_got, sq_msg, sq_got, st_got, turned,
    near_sem, in_sem, z_send, z_recv, f_send, c_send, c_recv, w1_send, w1_recv, w2_send, w2_recv, b_send, b_recv,
    d_send, d_recv, p_send, p_recv, r_send, r_recv, t_send, t_recv, s_send, s_recv,
):
    j = lax.axis_index("sp")
    t = lax.axis_index("tp")
    z, k = t // 2, t % 2
    quarter, i = z // 4, z % 4
    y, x = j // 4, j % 4
    sibling = 2 * z + 1 - k

    def at_sp(dy, dx):
        return lax.rem(y + dy, 4) * 4 + lax.rem(x + dx, 4)

    def ahead(dz):
        return lax.rem(z + dz, N_Z)

    barrier = pltpu.get_barrier_semaphore()
    pl.semaphore_signal(barrier, inc=1, device_id=(j, sibling), device_id_type=MESH)
    beside = (at_sp(0, 1), at_sp(0, 3))
    across = (at_sp(1, 0), at_sp(3, 0))
    for other in beside + across:
        pl.semaphore_signal(barrier, inc=1, device_id=(other, t), device_id_type=MESH)
    for dz in range(1, N_Z):
        pl.semaphore_signal(barrier, inc=1, device_id=(j, 2 * ahead(dz) + k), device_id_type=MESH)

    def rows_of(src_z, core):
        return pl.ds(pl.multiple_of((2 * src_z + core) * FEATS, FEATS), FEATS)

    def group_of(q):
        return pl.ds(pl.multiple_of(q * ROWS, ROWS), ROWS)

    my_lanes = pl.ds(pl.multiple_of(j * 128, 128), 128)

    loads = [
        pltpu.make_async_copy(src, dst, in_sem.at[n])
        for n, (src, dst) in enumerate(
            [
                (x_hbm, xs), (gain_hbm, gain_ref), (wk_hbm, wk_ref), (wd_hbm, wd_ref), (bias_hbm, bias_ref),
                (q_hbm, q_ref), (x_hbm.at[:, group_of(quarter)], xt.at[rows_of(z, k), :]),
                (wv_hbm, wv_ref), (drift_hbm, drift_ref), (og_hbm, og_ref),
            ]
        )
    ]
    for load in loads:
        load.start()
    for load in loads[:7]:
        load.wait()
    gain = gain_ref[...]
    wrel[0, 0:CH, :] = (wk_ref[...].astype(jnp.float32) * gain).astype(jnp.bfloat16)
    wrel[0, CH : 2 * CH, :] = (wd_ref[...].astype(jnp.float32) * gain).astype(jnp.bfloat16)
    small_msg[...] = jnp.zeros((2, 128), jnp.float32)
    small_msg[0:1, 0:CH] = bias_ref[...]
    small_msg[1:2, 0:CH] = q_ref[...].astype(jnp.float32) * KEY_CHANNELS ** (-0.5)
    pl.semaphore_wait(barrier, 5 + N_Z - 1)

    def pass_on(phase, others):
        for other in others:
            pl.semaphore_signal(near_sem.at[phase], inc=1, device_id=(other, t), device_id_type=MESH)

    pass_on(0, beside)

    def weights_along(n):
        return pltpu.make_async_remote_copy(
            src_ref=wrel.at[0, :, my_lanes], dst_ref=wrel.at[4 - n, :, my_lanes],
            send_sem=w1_send.at[n], recv_sem=w1_recv.at[4 - n],
            device_id=(j, 2 * ahead(4 * n) + k), device_id_type=MESH,
        )

    def weights_there(n):
        return pltpu.make_async_remote_copy(
            src_ref=wrel.at[0, :, my_lanes], dst_ref=wrel.at[n, :, my_lanes],
            send_sem=w1_send.at[n], recv_sem=w1_recv.at[n],
            device_id=(j, 2 * ahead(4 * n) + k), device_id_type=MESH,
        )

    def small_along(n):
        return pltpu.make_async_remote_copy(
            src_ref=small_msg, dst_ref=small_got.at[quarter],
            send_sem=b_send.at[n], recv_sem=b_recv.at[4 - n],
            device_id=(j, 2 * ahead(4 * n) + k), device_id_type=MESH,
        )

    def weights_across(o):
        return pltpu.make_async_remote_copy(
            src_ref=wrel.at[pl.ds(1, 3), :, my_lanes], dst_ref=wrel.at[pl.ds(1, 3), :, my_lanes],
            send_sem=w2_send.at[o], recv_sem=w2_recv.at[o],
            device_id=(at_sp(o // 4, o % 4), t), device_id_type=MESH,
        )

    def send_block(source, src_z, dst_z, sem):
        return pltpu.make_async_remote_copy(
            src_ref=source, dst_ref=xt.at[rows_of(src_z, k), :], send_sem=sem, recv_sem=z_recv.at[src_z],
            device_id=(j, 2 * dst_z + k), device_id_type=MESH,
        )

    nxt, opp, prv = lax.rem(quarter + 1, 4), lax.rem(quarter + 2, 4), lax.rem(quarter + 3, 4)
    own_sends = [
        send_block(xs.at[:, group_of(quarter)], z, ahead(1), z_send.at[0]),
        send_block(xs.at[:, group_of(quarter)], z, ahead(N_Z - 1), z_send.at[1]),
        send_block(xs.at[:, group_of(nxt)], z, 4 * nxt, z_send.at[2]),
        send_block(xs.at[:, group_of(prv)], z, 4 * prv + 3, z_send.at[3]),
        send_block(xs.at[:, group_of(opp)], z, 4 * opp + jnp.where(i >= 2, 0, 3), z_send.at[4]),
    ]
    for n in (2, 1, 3):
        weights_along(n).start()

    @pl.when(i < 3)
    def _():
        own_sends[0].start()

    @pl.when(i > 0)
    def _():
        own_sends[1].start()

    for send in own_sends[2:]:
        send.start()

    def to_core(src_z, way, n):
        place = xt.at[rows_of(src_z, k), :]
        return pltpu.make_async_remote_copy(
            src_ref=place, dst_ref=place, send_sem=c_send.at[way, n], recv_sem=c_recv.at[way, n],
            device_id=(j, sibling), device_id_type=MESH,
        )

    to_core(z, 0, STEPS).start()
    for n in (2, 1, 3):
        small_along(n).start()
    small_got[quarter] = small_msg[...]
    for load in loads[7:]:
        load.wait()

    def source(way, n):
        if n < 3:
            return lax.rem(z - (n + 1) + N_Z, N_Z) if way == 0 else ahead(n + 1)
        e = n - 3
        if e < 4:
            return 4 * prv + 3 - e if way == 0 else 4 * nxt + e
        return 4 * opp + 3 - (e - 4) if way == 0 else 4 * opp + e - 4

    def here(way, n):
        return i >= n + 1 if way == 0 else i + n + 1 <= 3

    def when_here(way, n, action):
        if n < 3:
            pl.when(here(way, n))(action)
        else:
            action()

    def onward(way, n):
        src = source(way, n)
        return send_block(xt.at[rows_of(src, k), :], src, ahead(1 if way == 0 else N_Z - 1), f_send.at[way, n])

    def goes_on(way):
        return i < 3 if way == 0 else i > 0

    def take(way, n):
        def action():
            src = source(way, n)
            place = xt.at[rows_of(src, k), :]
            pltpu.make_async_remote_copy(
                src_ref=place, dst_ref=place, send_sem=f_send.at[way, n], recv_sem=z_recv.at[src],
                device_id=(j, sibling), device_id_type=MESH,
            ).wait_recv()

            @pl.when(goes_on(way))
            def _():
                onward(way, n).start()

            to_core(src, way, n).start()

        when_here(way, n, action)

    def feats_of(src_z):
        return pl.ds(pl.multiple_of(src_z * 2 * FEATS, 2 * FEATS), 2 * FEATS)

    def compute(src_z, first=False):
        feats = feats_of(src_z)
        w = (wv_ref[feats, :].astype(jnp.float32).T * gain_ref[:, feats]).astype(jnp.bfloat16)
        block = xt[feats, :]
        term = jnp.dot(w, block, preferred_element_type=jnp.float32)
        wide = block.astype(jnp.float32)
        sq = jnp.sum((wide * wide).reshape(2 * FEATS // 8, 8, ROWS), axis=0)
        if first:
            acc[...] = term
            squares[...] = sq
        else:
            acc[...] += term
            squares[...] += sq

    def process(way, n):
        def action():
            src = source(way, n)
            to_core(src, way, n).wait_recv()
            compute(src)

        when_here(way, n, action)

    for n in range(STEPS):
        for way in range(2):
            take(way, n)
        if n == 0:
            to_core(z, 0, STEPS).wait_recv()
            compute(z, True)
        else:
            for way in range(2):
                process(way, n - 1)
        if n in (1, 2, 3):
            phase = n - 1
            pl.semaphore_wait(near_sem.at[phase], 2)
            if phase < 2:
                pass_on(phase + 1, across)
        if n == 4:
            for m in range(1, 4):
                weights_there(m).wait_recv()
            for o in SP_ORDER:
                weights_across(o).start()
    for n in range(1, 4):
        small_along(n).wait_recv()
    bias = jnp.concatenate([column_of(small_got[b, 0:1, 0:CH]) for b in range(4)], axis=0)
    q_rows = jnp.concatenate([small_got[b, 1:2, 0:CH] for b in range(4)] + [jnp.zeros((4, CH), jnp.float32)], axis=0)
    q_row = lane_row(q_rows)
    og_row = lane_row(jnp.concatenate([og_ref[...], jnp.zeros((4, VT), jnp.float32)], axis=0))
    row_at = lax.broadcasted_iota(jnp.int32, (128, 256), 0)
    col_at = lax.broadcasted_iota(jnp.int32, (128, 256), 1)
    summing = jnp.where((row_at > col_at) | (col_at >= 128), 1.0, 0.0).astype(jnp.bfloat16)
    for o in SP_ORDER:
        weights_across(o).wait_recv()
    for way in range(2):
        process(way, STEPS - 1)

    inverse = lax.rsqrt(jnp.sum(squares[...], axis=0, keepdims=True) * (1.0 / MODEL) + EPS)
    both = jnp.dot(wrel[...].reshape(4 * 2 * CH, MODEL), xt[...], preferred_element_type=jnp.float32)
    both = (both * inverse).astype(jnp.bfloat16).astype(jnp.float32)
    for m in range(4):
        b = lax.rem(quarter + m, 4)
        key_scr[b] = both[2 * CH * m : 2 * CH * m + CH]
        gate_scr[b] = both[2 * CH * m + CH : 2 * CH * m + 2 * CH]
    key = key_scr[...].reshape(NCH, ROWS)
    u = gate_scr[...].reshape(NCH, ROWS) + bias + drift_ref[:, group_of(quarter)]
    log_decay = (jnp.minimum(u, 0.0) - jnp.log1p(jnp.exp(-jnp.abs(u)))) * (1.0 / GATE_NORM)
    blocks = ROWS // 128
    stacked = jnp.concatenate([log_decay[:, 128 * b : 128 * b + 128] for b in range(blocks)], axis=0)
    high = stacked.astype(jnp.bfloat16)
    left = stacked - high.astype(jnp.float32)
    mid = left.astype(jnp.bfloat16)
    low = (left - mid.astype(jnp.float32)).astype(jnp.bfloat16)
    summed = (
        jnp.dot(low, summing, preferred_element_type=jnp.float32)
        + jnp.dot(mid, summing, preferred_element_type=jnp.float32)
        + jnp.dot(high, summing, preferred_element_type=jnp.float32)
    )
    rests = [None] * blocks
    run = jnp.zeros((NCH, 128), jnp.float32)
    for b in reversed(range(blocks)):
        rests[b] = summed[NCH * b : NCH * b + NCH, 0:128] + run
        run = run + summed[NCH * b : NCH * b + NCH, 128:256]
    d_msg[...] = run.T[0:1, :]

    def decays(o):
        return pltpu.make_async_remote_copy(
            src_ref=d_msg, dst_ref=d_got.at[4 * j + quarter], send_sem=d_send.at[o], recv_sem=d_recv.at[o],
            device_id=(at_sp((o % 16) // 4, o % 4), 2 * ahead(4 * (o // 16)) + k), device_id_type=MESH,
        )

    for o in ALL_ORDER:
        decays(o).start()
    d_got[4 * j + quarter] = d_msg[...]
    weighted = jnp.concatenate(
        [(key[:, 128 * b : 128 * b + 128] * jnp.exp(rests[b])).astype(jnp.bfloat16) for b in range(blocks)], axis=1
    )
    value = (acc[...] * inverse).astype(jnp.bfloat16)
    partial = lax.dot_general(value, weighted, (((1,), (1,)), ((), ())), preferred_element_type=jnp.float32)
    msg[...] = partial.reshape(N_SP, VT, NCH)

    def exchange(o):
        to = at_sp(o // 4, o % 4)
        return pltpu.make_async_remote_copy(
            src_ref=msg.at[to], dst_ref=got.at[j], send_sem=p_send.at[o], recv_sem=p_recv.at[o],
            device_id=(to, t), device_id_type=MESH,
        )

    for o in SP_ORDER:
        exchange(o).start()
    got[j] = msg[j]

    for way in range(2):
        for n in range(STEPS):
            def action(way=way, n=n):
                @pl.when(goes_on(way))
                def _():
                    onward(way, n).wait_send()

                to_core(source(way, n), way, n).wait_send()

            when_here(way, n, action)
    to_core(z, 0, STEPS).wait_send()

    @pl.when(i < 3)
    def _():
        own_sends[0].wait_send()

    @pl.when(i > 0)
    def _():
        own_sends[1].wait_send()

    for send in own_sends[2:]:
        send.wait_send()
    for n in range(1, 4):
        weights_along(n).wait_send()
        small_along(n).wait_send()
    for o in SP_ORDER:
        weights_across(o).wait_send()

    for o in SP_ORDER:
        exchange(o).wait_recv()
    for o in reversed(ALL_ORDER):
        decays(o).wait_recv()
    later = jnp.zeros((1, NCH), jnp.float32)
    state = jnp.zeros((VT, NCH), jnp.float32)
    for n in reversed(range(N_SP)):
        mine = later
        for g in range(4):
            piece = d_got[4 * n + g]
            mine = mine + jnp.where(g > quarter, piece, 0.0)
            later = later + piece
        state = state + jnp.exp(mine) * got[n]
    lane_head = lax.broadcasted_iota(jnp.int32, (8, 128), 1) // VT
    pick_head = jnp.where(lane_head == lax.broadcasted_iota(jnp.int32, (8, 128), 0), 1.0, 0.0)
    head_rows = lax.dot_general(
        pick_head, state * q_row, (((1,), (1,)), ((), ())), precision=HIGH, preferred_element_type=jnp.float32
    )
    read_msg[...] = lane_row(head_rows)

    def tell(o):
        return pltpu.make_async_remote_copy(
            src_ref=read_msg, dst_ref=read_got.at[t], send_sem=r_send.at[o], recv_sem=r_recv.at[o],
            device_id=(j, 2 * ahead(o // 2) + lax.rem(k + o % 2, 2)), device_id_type=MESH,
        )

    for o in TP_ORDER:
        tell(o).start()
    st_got[0] = state

    def states(n):
        return pltpu.make_async_remote_copy(
            src_ref=st_got.at[0], dst_ref=st_got.at[4 - n], send_sem=t_send.at[n], recv_sem=t_recv.at[4 - n],
            device_id=(j, 2 * ahead(4 * n) + k), device_id_type=MESH,
        )

    for n in (2, 1, 3):
        states(n).start()
    read_got[t] = read_msg[...]
    for o in SP_ORDER:
        exchange(o).wait_send()
    for o in ALL_ORDER:
        decays(o).wait_send()
    for o in TP_ORDER:
        tell(o).wait_recv()
    read = read_got[0]
    for n in range(1, N_TP):
        read = read + read_got[n]
    lane_group = lax.broadcasted_iota(jnp.int32, (1, 128), 1) // VT
    sq = jnp.zeros((1, 128), jnp.float32)
    for h in range(HEADS):
        own = jnp.sum(jnp.where(lane_group == h, read * read, 0.0), axis=1, keepdims=True)
        sq = jnp.where(lane_group == h, jnp.broadcast_to(own, (1, 128)), sq)
    sq_msg[...] = sq

    def share(o):
        return pltpu.make_async_remote_copy(
            src_ref=sq_msg, dst_ref=sq_got.at[j], send_sem=s_send.at[o], recv_sem=s_recv.at[o],
            device_id=(at_sp(o // 4, o % 4), t), device_id_type=MESH,
        )

    for o in SP_ORDER:
        share(o).start()
    sq_got[j] = sq_msg[...]
    for n in range(1, 4):
        states(n).wait_recv()
    total = st_got[0] + st_got[1] + st_got[2] + st_got[3]
    turned[...] = jnp.concatenate([total] * 4, axis=0).T
    out_ref[0:CH, :] = turned[pl.ds(pl.multiple_of(CH * quarter, CH), CH), :]
    for n in range(1, 4):
        states(n).wait_send()
    for o in TP_ORDER:
        tell(o).wait_send()
    for o in SP_ORDER:
        share(o).wait_recv()
    whole = sq_got[0]
    for n in range(1, N_SP):
        whole = whole + sq_got[n]
    out_ref[CH : CH + 1, :] = read * lax.rsqrt(whole * (1.0 / VALS) + EPS) * og_row
    for o in SP_ORDER:
        share(o).wait_send()


def unpack(packed_ref, state_ref, read_ref):
    state_ref[...] = packed_ref[0:CH, 0:VT].astype(jnp.bfloat16)
    for h in range(HEADS):
        read_ref[h : h + 1, :] = packed_ref[CH : CH + 1, VT * h : VT * h + VT]


def body(tokens, norm_gain, w_key, w_decay, w_value, decay_bias, gate_drift, queries, out_gain):
    dma = pltpu.SemaphoreType.DMA
    vmem = pl.BlockSpec(memory_space=pltpu.VMEM)
    f32, bf16 = jnp.float32, jnp.bfloat16
    packed = pl.pallas_call(
        kernel,
        out_shape=jax.ShapeDtypeStruct((CH + 8, 128), f32),
        in_specs=[pl.BlockSpec(memory_space=pl.ANY)] * 9,
        out_specs=vmem,
        scratch_shapes=[
            pltpu.VMEM((FEATS, SPAN), bf16),
            pltpu.VMEM((MODEL, ROWS), bf16),
            pltpu.VMEM((1, MODEL), f32),
            pltpu.VMEM((CH, MODEL), bf16),
            pltpu.VMEM((CH, MODEL), bf16),
            pltpu.VMEM((MODEL, VALS), bf16),
            pltpu.VMEM((1, CH), f32),
            pltpu.VMEM((1, SPAN), f32),
            pltpu.VMEM((1, CH), bf16),
            pltpu.VMEM((HEADS, VT), f32),
            pltpu.VMEM((4, 2 * CH, MODEL), bf16),
            pltpu.VMEM((VALS, ROWS), f32),
            pltpu.VMEM((8, ROWS), f32),
            pltpu.VMEM((2, 128), f32),
            pltpu.VMEM((4, 2, 128), f32),
            pltpu.VMEM((4, CH, ROWS), f32),
            pltpu.VMEM((4, CH, ROWS), f32),
            pltpu.VMEM((N_SP, VT, NCH), f32),
            pltpu.VMEM((N_SP, VT, NCH), f32),
            pltpu.VMEM((1, 128), f32),
            pltpu.VMEM((4 * N_SP, 1, 128), f32),
            pltpu.VMEM((1, 128), f32),
            pltpu.VMEM((N_TP, 1, 128), f32),
            pltpu.VMEM((1, 128), f32),
            pltpu.VMEM((N_SP, 1, 128), f32),
            pltpu.VMEM((4, VT, NCH), f32),
            pltpu.VMEM((128, 128), f32),
            pltpu.SemaphoreType.REGULAR((3,)), dma((10,)), dma((5,)), dma((N_Z,)), dma((2, STEPS)),
            dma((2, STEPS + 1)), dma((2, STEPS + 1)), dma((4,)), dma((4,)), dma((N_SP,)), dma((N_SP,)), dma((4,)), dma((4,)),
            dma((64,)), dma((64,)), dma((N_SP,)), dma((N_SP,)), dma((N_TP,)), dma((N_TP,)), dma((4,)), dma((4,)),
            dma((N_SP,)), dma((N_SP,)),
        ],
        compiler_params=pltpu.CompilerParams(
            collective_id=0, has_side_effects=True, vmem_limit_bytes=67043328
        ),
    )(
        tokens.T, norm_gain.reshape(1, MODEL), w_key.T, w_decay.T, w_value, decay_bias.reshape(1, CH),
        gate_drift.reshape(1, SPAN), queries.reshape(1, CH), out_gain,
    )
    return pl.pallas_call(
        unpack,
        out_shape=(jax.ShapeDtypeStruct((CH, VT), bf16), jax.ShapeDtypeStruct((HEADS, VT), f32)),
        in_specs=[vmem],
        out_specs=(vmem, vmem),
    )(packed)


def solution(mesh):
    return jax.shard_map(
        body,
        mesh=mesh,
        in_specs=(
            P("sp", "tp"), P(), P(None, "tp"), P(None, "tp"), P(), P("tp"), P("sp"), P("tp"), P(None, "sp"),
        ),
        out_specs=(P("tp", "sp"), P(None, "sp")),
        check_vma=False,
    )
```

```python
import jax
import jax.numpy as jnp
from jax import lax
from jax.experimental import pallas as pl
from jax.experimental.pallas import tpu as pltpu
from jax.sharding import PartitionSpec as P

MESH = pl.DeviceIdType.MESH
EPS = 1e-06
GATE_NORM = 16.0
KEY_CHANNELS = 256
N_SP, N_TP, N_Z = 16, 32, 16
SPAN, FEATS, VALS, CH = 2048, 64, 512, 32
QUARTERS = 4
ROWS = SPAN // QUARTERS
NCH = QUARTERS * CH
VT = 32
HEADS = 4
MODEL = N_TP * FEATS
STEPS = 9
BEATS = 12
WEIGHT_BEAT = 4
HIGH = lax.Precision.HIGHEST


def hops(step, size):
    return min(step, size - step)


def sp_hops(o):
    return hops(o // 4, 4) + hops(o % 4, 4)


SP_ORDER = sorted(range(1, N_SP), key=lambda o: -sp_hops(o))
TP_ORDER = sorted(range(1, N_TP), key=lambda o: -hops(o // 2, N_Z))
ALL_ORDER = sorted(range(1, 4 * N_SP), key=lambda o: -(hops(4 * (o // 16), N_Z) + sp_hops(o % 16)))


def column_of(row):
    n = row.shape[1]
    on_diagonal = lax.broadcasted_iota(jnp.int32, (n, n), 0) == lax.broadcasted_iota(jnp.int32, (n, n), 1)
    return jnp.sum(jnp.where(on_diagonal, jnp.broadcast_to(row, (n, n)), 0.0), axis=1, keepdims=True)


def lane_row(rows):
    at = lax.broadcasted_iota(jnp.int32, (VT, 128), 1)
    pick = jnp.where(lax.rem(at, VT) == lax.broadcasted_iota(jnp.int32, (VT, 128), 0), 1.0, 0.0)
    wide = jnp.dot(rows, pick, precision=HIGH, preferred_element_type=jnp.float32)
    lane = lax.broadcasted_iota(jnp.int32, (8, 128), 1) // VT
    mine = lane == lax.broadcasted_iota(jnp.int32, (8, 128), 0)
    return jnp.sum(jnp.where(mine, wide, 0.0), axis=0, keepdims=True)


def kernel(
    x_hbm, gain_hbm, wk_hbm, wd_hbm, wv_hbm, bias_hbm, drift_hbm, q_hbm, og_hbm,
    out_ref,
    xs, xt, gain_ref, wk_ref, wd_ref, wv_ref, bias_ref, drift_ref, q_ref, og_ref,
    wrel, wvt, squares, small_msg, small_got, key_scr, gate_scr, msg, got, d_msg, d_got,
    read_msg, read_got, sq_msg, sq_got, st_got, turned,
    near_sem, in_sem, z_send, z_recv, f_send, c_send, c_recv, w1_send, w1_recv, w2_send, w2_recv, b_send, b_recv,
    d_send, d_recv, p_send, p_recv, r_send, r_recv, t_send, t_recv, s_send, s_recv,
):
    j = lax.axis_index("sp")
    t = lax.axis_index("tp")
    z, k = t // 2, t % 2
    quarter, i = z // 4, z % 4
    y, x = j // 4, j % 4
    sibling = 2 * z + 1 - k

    def at_sp(dy, dx):
        return lax.rem(y + dy, 4) * 4 + lax.rem(x + dx, 4)

    def ahead(dz):
        return lax.rem(z + dz, N_Z)

    barrier = pltpu.get_barrier_semaphore()
    pl.semaphore_signal(barrier, inc=1, device_id=(j, sibling), device_id_type=MESH)
    beside = (at_sp(0, 1), at_sp(0, 3))
    across = (at_sp(1, 0), at_sp(3, 0))
    for other in beside + across:
        pl.semaphore_signal(barrier, inc=1, device_id=(other, t), device_id_type=MESH)
    for dz in range(1, N_Z):
        pl.semaphore_signal(barrier, inc=1, device_id=(j, 2 * ahead(dz) + k), device_id_type=MESH)

    def rows_of(src_z, core):
        return pl.ds(pl.multiple_of((2 * src_z + core) * FEATS, FEATS), FEATS)

    def group_of(q):
        return pl.ds(pl.multiple_of(q * ROWS, ROWS), ROWS)

    my_lanes = pl.ds(pl.multiple_of(j * 128, 128), 128)

    loads = [
        pltpu.make_async_copy(src, dst, in_sem.at[n])
        for n, (src, dst) in enumerate(
            [
                (x_hbm, xs), (gain_hbm, gain_ref), (wk_hbm, wk_ref), (wd_hbm, wd_ref), (bias_hbm, bias_ref),
                (q_hbm, q_ref), (x_hbm.at[:, group_of(quarter)], xt.at[rows_of(z, k), :]),
                (wv_hbm, wv_ref), (drift_hbm, drift_ref), (og_hbm, og_ref),
            ]
        )
    ]
    for load in loads:
        load.start()
    for load in loads[:7]:
        load.wait()
    gain = gain_ref[...]
    wrel[0, 0] = (wk_ref[...].astype(jnp.float32) * gain).astype(jnp.bfloat16)
    wrel[1, 0] = (wd_ref[...].astype(jnp.float32) * gain).astype(jnp.bfloat16)
    small_msg[...] = jnp.zeros((2, 128), jnp.float32)
    small_msg[0:1, 0:CH] = bias_ref[...]
    small_msg[1:2, 0:CH] = q_ref[...].astype(jnp.float32) * KEY_CHANNELS ** (-0.5)
    pl.semaphore_wait(barrier, 5 + N_Z - 1)

    def pass_on(phase, others):
        for other in others:
            pl.semaphore_signal(near_sem.at[phase], inc=1, device_id=(other, t), device_id_type=MESH)

    pass_on(0, beside)

    def weights_along(n):
        return pltpu.make_async_remote_copy(
            src_ref=wrel.at[:, 0, :, my_lanes], dst_ref=wrel.at[:, 4 - n, :, my_lanes],
            send_sem=w1_send.at[n], recv_sem=w1_recv.at[4 - n],
            device_id=(j, 2 * ahead(4 * n) + k), device_id_type=MESH,
        )

    def weights_there(n):
        return pltpu.make_async_remote_copy(
            src_ref=wrel.at[:, 0, :, my_lanes], dst_ref=wrel.at[:, n, :, my_lanes],
            send_sem=w1_send.at[n], recv_sem=w1_recv.at[n],
            device_id=(j, 2 * ahead(4 * n) + k), device_id_type=MESH,
        )

    def small_along(n):
        return pltpu.make_async_remote_copy(
            src_ref=small_msg, dst_ref=small_got.at[quarter],
            send_sem=b_send.at[n], recv_sem=b_recv.at[4 - n],
            device_id=(j, 2 * ahead(4 * n) + k), device_id_type=MESH,
        )

    def weights_across(o):
        return pltpu.make_async_remote_copy(
            src_ref=wrel.at[:, pl.ds(1, 3), :, my_lanes], dst_ref=wrel.at[:, pl.ds(1, 3), :, my_lanes],
            send_sem=w2_send.at[o], recv_sem=w2_recv.at[o],
            device_id=(at_sp(o // 4, o % 4), t), device_id_type=MESH,
        )

    def send_block(source, src_z, dst_z, sem):
        return pltpu.make_async_remote_copy(
            src_ref=source, dst_ref=xt.at[rows_of(src_z, k), :], send_sem=sem, recv_sem=z_recv.at[src_z],
            device_id=(j, 2 * dst_z + k), device_id_type=MESH,
        )

    nxt, opp, prv = lax.rem(quarter + 1, 4), lax.rem(quarter + 2, 4), lax.rem(quarter + 3, 4)
    own_sends = [
        send_block(xs.at[:, group_of(quarter)], z, ahead(1), z_send.at[0]),
        send_block(xs.at[:, group_of(quarter)], z, ahead(N_Z - 1), z_send.at[1]),
        send_block(xs.at[:, group_of(nxt)], z, 4 * nxt, z_send.at[2]),
        send_block(xs.at[:, group_of(prv)], z, 4 * prv + 3, z_send.at[3]),
        send_block(xs.at[:, group_of(opp)], z, 4 * opp + jnp.where(i >= 2, 0, 3), z_send.at[4]),
    ]
    for n in (2, 1, 3):
        weights_along(n).start()

    @pl.when(i < 3)
    def _():
        own_sends[0].start()

    @pl.when(i > 0)
    def _():
        own_sends[1].start()

    for send in own_sends[2:]:
        send.start()

    def to_core(src_z, way, n):
        place = xt.at[rows_of(src_z, k), :]
        return pltpu.make_async_remote_copy(
            src_ref=place, dst_ref=place, send_sem=c_send.at[way, n], recv_sem=c_recv.at[way, n],
            device_id=(j, sibling), device_id_type=MESH,
        )

    to_core(z, 0, STEPS).start()
    for n in (2, 1, 3):
        small_along(n).start()
    small_got[quarter] = small_msg[...]
    for load in loads[7:]:
        load.wait()

    def behind(way):
        return i if way == 0 else 3 - i

    def source(way, n):
        e = n - behind(way)
        if way == 0:
            outside = jnp.where(e < 4, 4 * prv + 3 - e, 4 * opp + 7 - e)
            return jnp.where(e < 0, lax.rem(z - (n + 1) + 2 * N_Z, N_Z), outside)
        outside = jnp.where(e < 4, 4 * nxt + e, 4 * opp + e - 4)
        return jnp.where(e < 0, lax.rem(z + n + 1, N_Z), outside)

    def when_due(way, n, action):
        pl.when((n >= 0) & (n < 6 + behind(way)))(action)

    def onward(way, n):
        src = source(way, n)
        return send_block(xt.at[rows_of(src, k), :], src, ahead(1 if way == 0 else N_Z - 1), f_send.at[way, n])

    def goes_on(way):
        return i < 3 if way == 0 else i > 0

    def take(way, n):
        def action():
            src = source(way, n)
            place = xt.at[rows_of(src, k), :]
            pltpu.make_async_remote_copy(
                src_ref=place, dst_ref=place, send_sem=f_send.at[way, n], recv_sem=z_recv.at[src],
                device_id=(j, sibling), device_id_type=MESH,
            ).wait_recv()

            @pl.when(goes_on(way))
            def _():
                onward(way, n).start()

            to_core(src, way, n).start()

        when_due(way, n, action)

    def feats_of(src_z):
        return pl.ds(pl.multiple_of(src_z * 2 * FEATS, 2 * FEATS), 2 * FEATS)

    def compute(src_z, first=False):
        wide = xt[feats_of(src_z), :].astype(jnp.float32)
        sq = jnp.sum((wide * wide).reshape(2 * FEATS // 8, 8, ROWS), axis=0)
        if first:
            squares[...] = sq
        else:
            squares[...] += sq

    def prepare(n):
        feats = pl.ds(256 * n, 256)
        wvt[:, feats] = (wv_ref[feats, :].astype(jnp.float32).T * gain_ref[:, feats]).astype(jnp.bfloat16)

    def process(way, n):
        def action():
            src = source(way, n)
            to_core(src, way, n).wait_recv()
            compute(src)

        when_due(way, n, action)

    for n in range(BEATS):
        for way in range(2):
            take(way, n - behind(way))
        if n == 0:
            to_core(z, 0, STEPS).wait_recv()
            compute(z, True)
        else:
            for way in range(2):
                process(way, n - 1 - behind(way))
        if n < MODEL // 256:
            prepare(n)
        if n in (2, 3, 4):
            phase = n - 2
            pl.semaphore_wait(near_sem.at[phase], 2)
            if phase < 2:
                pass_on(phase + 1, across)
        if n == WEIGHT_BEAT:
            for m in range(1, 4):
                weights_there(m).wait_recv()
            for o in SP_ORDER:
                weights_across(o).start()
    for n in range(1, 4):
        small_along(n).wait_recv()
    bias = jnp.concatenate([column_of(small_got[b, 0:1, 0:CH]) for b in range(4)], axis=0)
    q_rows = jnp.concatenate([small_got[b, 1:2, 0:CH] for b in range(4)] + [jnp.zeros((4, CH), jnp.float32)], axis=0)
    q_row = lane_row(q_rows)
    og_row = lane_row(jnp.concatenate([og_ref[...], jnp.zeros((4, VT), jnp.float32)], axis=0))
    row_at = lax.broadcasted_iota(jnp.int32, (128, 256), 0)
    col_at = lax.broadcasted_iota(jnp.int32, (128, 256), 1)
    summing = jnp.where((row_at > col_at) | (col_at >= 128), 1.0, 0.0).astype(jnp.bfloat16)
    for o in SP_ORDER:
        weights_across(o).wait_recv()
    for way in range(2):
        process(way, BEATS - 1 - behind(way))

    inverse = lax.rsqrt(jnp.sum(squares[...], axis=0, keepdims=True) * (1.0 / MODEL) + EPS)
    gate = jnp.dot(wrel[1].reshape(NCH, MODEL), xt[...], preferred_element_type=jnp.float32)
    gate = (gate * inverse).astype(jnp.bfloat16).astype(jnp.float32)
    for m in range(4):
        gate_scr[lax.rem(quarter + m, 4)] = gate[CH * m : CH * m + CH]
    u = gate_scr[...].reshape(NCH, ROWS) + bias + drift_ref[:, group_of(quarter)]
    log_decay = (jnp.minimum(u, 0.0) - jnp.log1p(jnp.exp(-jnp.abs(u)))) * (1.0 / GATE_NORM)
    blocks = ROWS // 128
    stacked = jnp.concatenate([log_decay[:, 128 * b : 128 * b + 128] for b in range(blocks)], axis=0)
    high = stacked.astype(jnp.bfloat16)
    left = stacked - high.astype(jnp.float32)
    mid = left.astype(jnp.bfloat16)
    low = (left - mid.astype(jnp.float32)).astype(jnp.bfloat16)
    summed = (
        jnp.dot(low, summing, preferred_element_type=jnp.float32)
        + jnp.dot(mid, summing, preferred_element_type=jnp.float32)
        + jnp.dot(high, summing, preferred_element_type=jnp.float32)
    )
    rests = [None] * blocks
    run = jnp.zeros((NCH, 128), jnp.float32)
    for b in reversed(range(blocks)):
        rests[b] = summed[NCH * b : NCH * b + NCH, 0:128] + run
        run = run + summed[NCH * b : NCH * b + NCH, 128:256]
    d_msg[...] = run.T[0:1, :]

    def decays(o):
        return pltpu.make_async_remote_copy(
            src_ref=d_msg, dst_ref=d_got.at[4 * j + quarter], send_sem=d_send.at[o], recv_sem=d_recv.at[o],
            device_id=(at_sp((o % 16) // 4, o % 4), 2 * ahead(4 * (o // 16)) + k), device_id_type=MESH,
        )

    for o in ALL_ORDER:
        decays(o).start()
    d_got[4 * j + quarter] = d_msg[...]
    key = jnp.dot(wrel[0].reshape(NCH, MODEL), xt[...], preferred_element_type=jnp.float32)
    key = (key * inverse).astype(jnp.bfloat16).astype(jnp.float32)
    for m in range(4):
        key_scr[lax.rem(quarter + m, 4)] = key[CH * m : CH * m + CH]
    key = key_scr[...].reshape(NCH, ROWS)
    weighted = jnp.concatenate(
        [(key[:, 128 * b : 128 * b + 128] * jnp.exp(rests[b])).astype(jnp.bfloat16) for b in range(blocks)], axis=1
    )
    value = jnp.dot(wvt[...], xt[...], preferred_element_type=jnp.float32)
    value = (value * inverse).astype(jnp.bfloat16)
    partial = lax.dot_general(value, weighted, (((1,), (1,)), ((), ())), preferred_element_type=jnp.float32)
    msg[...] = partial.reshape(N_SP, VT, NCH)

    def exchange(o):
        to = at_sp(o // 4, o % 4)
        return pltpu.make_async_remote_copy(
            src_ref=msg.at[to], dst_ref=got.at[j], send_sem=p_send.at[o], recv_sem=p_recv.at[o],
            device_id=(to, t), device_id_type=MESH,
        )

    for o in SP_ORDER:
        exchange(o).start()
    got[j] = msg[j]

    for way in range(2):
        for n in range(STEPS):
            def action(way=way, n=n):
                @pl.when(goes_on(way))
                def _():
                    onward(way, n).wait_send()

                to_core(source(way, n), way, n).wait_send()

            when_due(way, n, action)
    to_core(z, 0, STEPS).wait_send()

    @pl.when(i < 3)
    def _():
        own_sends[0].wait_send()

    @pl.when(i > 0)
    def _():
        own_sends[1].wait_send()

    for send in own_sends[2:]:
        send.wait_send()
    for n in range(1, 4):
        weights_along(n).wait_send()
        small_along(n).wait_send()
    for o in SP_ORDER:
        weights_across(o).wait_send()

    for o in SP_ORDER:
        exchange(o).wait_recv()
    for o in reversed(ALL_ORDER):
        decays(o).wait_recv()
    later = jnp.zeros((1, NCH), jnp.float32)
    state = jnp.zeros((VT, NCH), jnp.float32)
    for n in reversed(range(N_SP)):
        mine = later
        for g in range(4):
            piece = d_got[4 * n + g]
            mine = mine + jnp.where(g > quarter, piece, 0.0)
            later = later + piece
        state = state + jnp.exp(mine) * got[n]
    lane_head = lax.broadcasted_iota(jnp.int32, (8, 128), 1) // VT
    pick_head = jnp.where(lane_head == lax.broadcasted_iota(jnp.int32, (8, 128), 0), 1.0, 0.0)
    head_rows = lax.dot_general(
        pick_head, state * q_row, (((1,), (1,)), ((), ())), precision=HIGH, preferred_element_type=jnp.float32
    )
    read_msg[...] = lane_row(head_rows)

    def tell(o):
        return pltpu.make_async_remote_copy(
            src_ref=read_msg, dst_ref=read_got.at[t], send_sem=r_send.at[o], recv_sem=r_recv.at[o],
            device_id=(j, 2 * ahead(o // 2) + lax.rem(k + o % 2, 2)), device_id_type=MESH,
        )

    for o in TP_ORDER:
        tell(o).start()
    st_got[0] = state

    def states(n):
        return pltpu.make_async_remote_copy(
            src_ref=st_got.at[0], dst_ref=st_got.at[4 - n], send_sem=t_send.at[n], recv_sem=t_recv.at[4 - n],
            device_id=(j, 2 * ahead(4 * n) + k), device_id_type=MESH,
        )

    for n in (2, 1, 3):
        states(n).start()
    read_got[t] = read_msg[...]
    for o in SP_ORDER:
        exchange(o).wait_send()
    for o in ALL_ORDER:
        decays(o).wait_send()
    for o in TP_ORDER:
        tell(o).wait_recv()
    read = read_got[0]
    for n in range(1, N_TP):
        read = read + read_got[n]
    lane_group = lax.broadcasted_iota(jnp.int32, (1, 128), 1) // VT
    sq = jnp.zeros((1, 128), jnp.float32)
    for h in range(HEADS):
        own = jnp.sum(jnp.where(lane_group == h, read * read, 0.0), axis=1, keepdims=True)
        sq = jnp.where(lane_group == h, jnp.broadcast_to(own, (1, 128)), sq)
    sq_msg[...] = sq

    def share(o):
        return pltpu.make_async_remote_copy(
            src_ref=sq_msg, dst_ref=sq_got.at[j], send_sem=s_send.at[o], recv_sem=s_recv.at[o],
            device_id=(at_sp(o // 4, o % 4), t), device_id_type=MESH,
        )

    for o in SP_ORDER:
        share(o).start()
    sq_got[j] = sq_msg[...]
    for n in range(1, 4):
        states(n).wait_recv()
    total = st_got[0] + st_got[1] + st_got[2] + st_got[3]
    turned[...] = jnp.concatenate([total] * 4, axis=0).T
    out_ref[0:CH, :] = turned[pl.ds(pl.multiple_of(CH * quarter, CH), CH), :]
    for n in range(1, 4):
        states(n).wait_send()
    for o in TP_ORDER:
        tell(o).wait_send()
    for o in SP_ORDER:
        share(o).wait_recv()
    whole = sq_got[0]
    for n in range(1, N_SP):
        whole = whole + sq_got[n]
    out_ref[CH : CH + 1, :] = read * lax.rsqrt(whole * (1.0 / VALS) + EPS) * og_row
    for o in SP_ORDER:
        share(o).wait_send()


def unpack(packed_ref, state_ref, read_ref):
    state_ref[...] = packed_ref[0:CH, 0:VT].astype(jnp.bfloat16)
    for h in range(HEADS):
        read_ref[h : h + 1, :] = packed_ref[CH : CH + 1, VT * h : VT * h + VT]


def body(tokens, norm_gain, w_key, w_decay, w_value, decay_bias, gate_drift, queries, out_gain):
    dma = pltpu.SemaphoreType.DMA
    vmem = pl.BlockSpec(memory_space=pltpu.VMEM)
    f32, bf16 = jnp.float32, jnp.bfloat16
    packed = pl.pallas_call(
        kernel,
        out_shape=jax.ShapeDtypeStruct((CH + 8, 128), f32),
        in_specs=[pl.BlockSpec(memory_space=pl.ANY)] * 9,
        out_specs=vmem,
        scratch_shapes=[
            pltpu.VMEM((FEATS, SPAN), bf16),
            pltpu.VMEM((MODEL, ROWS), bf16),
            pltpu.VMEM((1, MODEL), f32),
            pltpu.VMEM((CH, MODEL), bf16),
            pltpu.VMEM((CH, MODEL), bf16),
            pltpu.VMEM((MODEL, VALS), bf16),
            pltpu.VMEM((1, CH), f32),
            pltpu.VMEM((1, SPAN), f32),
            pltpu.VMEM((1, CH), bf16),
            pltpu.VMEM((HEADS, VT), f32),
            pltpu.VMEM((2, 4, CH, MODEL), bf16),
            pltpu.VMEM((VALS, MODEL), bf16),
            pltpu.VMEM((8, ROWS), f32),
            pltpu.VMEM((2, 128), f32),
            pltpu.VMEM((4, 2, 128), f32),
            pltpu.VMEM((4, CH, ROWS), f32),
            pltpu.VMEM((4, CH, ROWS), f32),
            pltpu.VMEM((N_SP, VT, NCH), f32),
            pltpu.VMEM((N_SP, VT, NCH), f32),
            pltpu.VMEM((1, 128), f32),
            pltpu.VMEM((4 * N_SP, 1, 128), f32),
            pltpu.VMEM((1, 128), f32),
            pltpu.VMEM((N_TP, 1, 128), f32),
            pltpu.VMEM((1, 128), f32),
            pltpu.VMEM((N_SP, 1, 128), f32),
            pltpu.VMEM((4, VT, NCH), f32),
            pltpu.VMEM((128, 128), f32),
            pltpu.SemaphoreType.REGULAR((3,)), dma((10,)), dma((5,)), dma((N_Z,)), dma((2, STEPS)),
            dma((2, STEPS + 1)), dma((2, STEPS + 1)), dma((4,)), dma((4,)), dma((N_SP,)), dma((N_SP,)), dma((4,)), dma((4,)),
            dma((64,)), dma((64,)), dma((N_SP,)), dma((N_SP,)), dma((N_TP,)), dma((N_TP,)), dma((4,)), dma((4,)),
            dma((N_SP,)), dma((N_SP,)),
        ],
        compiler_params=pltpu.CompilerParams(
            collective_id=0, has_side_effects=True, vmem_limit_bytes=67043328
        ),
    )(
        tokens.T, norm_gain.reshape(1, MODEL), w_key.T, w_decay.T, w_value, decay_bias.reshape(1, CH),
        gate_drift.reshape(1, SPAN), queries.reshape(1, CH), out_gain,
    )
    return pl.pallas_call(
        unpack,
        out_shape=(jax.ShapeDtypeStruct((CH, VT), bf16), jax.ShapeDtypeStruct((HEADS, VT), f32)),
        in_specs=[vmem],
        out_specs=(vmem, vmem),
    )(packed)


def solution(mesh):
    return jax.shard_map(
        body,
        mesh=mesh,
        in_specs=(
            P("sp", "tp"), P(), P(None, "tp"), P(None, "tp"), P(), P("tp"), P("sp"), P("tp"), P(None, "sp"),
        ),
        out_specs=(P("tp", "sp"), P(None, "sp")),
        check_vma=False,
    )
```

```python
import jax
import jax.numpy as jnp
from jax import lax
from jax.experimental import pallas as pl
from jax.experimental.pallas import tpu as pltpu
from jax.sharding import PartitionSpec as P

MESH = pl.DeviceIdType.MESH
EPS = 1e-06
GATE_NORM = 16.0
KEY_CHANNELS = 256
N_SP, N_TP, N_Z = 16, 32, 16
SPAN, FEATS, VALS, CH = 2048, 64, 512, 32
QUARTERS = 4
ROWS = SPAN // QUARTERS
NCH = QUARTERS * CH
VT = 32
HEADS = 4
MODEL = N_TP * FEATS
STEPS = 9
LAG = 2
DEFER = 2
BEATS = 9 + 3 * LAG
WEIGHT_BEAT = 4
HIGH = lax.Precision.HIGHEST


def hops(step, size):
    return min(step, size - step)


def sp_hops(o):
    return hops(o // 4, 4) + hops(o % 4, 4)


SP_ORDER = sorted(range(1, N_SP), key=lambda o: -sp_hops(o))
TP_ORDER = sorted(range(1, N_TP), key=lambda o: -hops(o // 2, N_Z))
ALL_ORDER = sorted(range(1, 4 * N_SP), key=lambda o: -(hops(4 * (o // 16), N_Z) + sp_hops(o % 16)))


def column_of(row):
    n = row.shape[1]
    on_diagonal = lax.broadcasted_iota(jnp.int32, (n, n), 0) == lax.broadcasted_iota(jnp.int32, (n, n), 1)
    return jnp.sum(jnp.where(on_diagonal, jnp.broadcast_to(row, (n, n)), 0.0), axis=1, keepdims=True)


def lane_row(rows):
    at = lax.broadcasted_iota(jnp.int32, (VT, 128), 1)
    pick = jnp.where(lax.rem(at, VT) == lax.broadcasted_iota(jnp.int32, (VT, 128), 0), 1.0, 0.0)
    wide = jnp.dot(rows, pick, precision=HIGH, preferred_element_type=jnp.float32)
    lane = lax.broadcasted_iota(jnp.int32, (8, 128), 1) // VT
    mine = lane == lax.broadcasted_iota(jnp.int32, (8, 128), 0)
    return jnp.sum(jnp.where(mine, wide, 0.0), axis=0, keepdims=True)


def kernel(
    x_hbm, gain_hbm, wk_hbm, wd_hbm, wv_hbm, bias_hbm, drift_hbm, q_hbm, og_hbm,
    out_ref,
    xs, xt, gain_ref, wk_ref, wd_ref, wv_ref, bias_ref, drift_ref, q_ref, og_ref,
    wrel, wvt, squares, small_msg, small_got, key_scr, gate_scr, msg, got, d_msg, d_got,
    read_msg, read_got, sq_msg, sq_got, st_got, turned,
    near_sem, in_sem, z_send, z_recv, f_send, c_send, c_recv, w1_send, w1_recv, w2_send, w2_recv, b_send, b_recv,
    d_send, d_recv, p_send, p_recv, r_send, r_recv, t_send, t_recv, s_send, s_recv,
):
    j = lax.axis_index("sp")
    t = lax.axis_index("tp")
    z, k = t // 2, t % 2
    quarter, i = z // 4, z % 4
    y, x = j // 4, j % 4
    sibling = 2 * z + 1 - k

    def at_sp(dy, dx):
        return lax.rem(y + dy, 4) * 4 + lax.rem(x + dx, 4)

    def ahead(dz):
        return lax.rem(z + dz, N_Z)

    barrier = pltpu.get_barrier_semaphore()
    pl.semaphore_signal(barrier, inc=1, device_id=(j, sibling), device_id_type=MESH)
    beside = (at_sp(0, 1), at_sp(0, 3))
    across = (at_sp(1, 0), at_sp(3, 0))
    for other in beside + across:
        pl.semaphore_signal(barrier, inc=1, device_id=(other, t), device_id_type=MESH)
    for dz in range(1, N_Z):
        pl.semaphore_signal(barrier, inc=1, device_id=(j, 2 * ahead(dz) + k), device_id_type=MESH)

    def rows_of(src_z, core):
        return pl.ds(pl.multiple_of((2 * src_z + core) * FEATS, FEATS), FEATS)

    def group_of(q):
        return pl.ds(pl.multiple_of(q * ROWS, ROWS), ROWS)

    my_lanes = pl.ds(pl.multiple_of(j * 128, 128), 128)

    loads = [
        pltpu.make_async_copy(src, dst, in_sem.at[n])
        for n, (src, dst) in enumerate(
            [
                (x_hbm, xs), (gain_hbm, gain_ref), (wk_hbm, wk_ref), (wd_hbm, wd_ref), (bias_hbm, bias_ref),
                (q_hbm, q_ref), (x_hbm.at[:, group_of(quarter)], xt.at[rows_of(z, k), :]),
                (wv_hbm, wv_ref), (drift_hbm, drift_ref), (og_hbm, og_ref),
            ]
        )
    ]
    for load in loads:
        load.start()
    for load in loads[:7]:
        load.wait()
    gain = gain_ref[...]
    wrel[0, 0] = (wk_ref[...].astype(jnp.float32) * gain).astype(jnp.bfloat16)
    wrel[1, 0] = (wd_ref[...].astype(jnp.float32) * gain).astype(jnp.bfloat16)
    small_msg[...] = jnp.zeros((2, 128), jnp.float32)
    small_msg[0:1, 0:CH] = bias_ref[...]
    small_msg[1:2, 0:CH] = q_ref[...].astype(jnp.float32) * KEY_CHANNELS ** (-0.5)
    pl.semaphore_wait(barrier, 5 + N_Z - 1)

    def pass_on(phase, others):
        for other in others:
            pl.semaphore_signal(near_sem.at[phase], inc=1, device_id=(other, t), device_id_type=MESH)

    pass_on(0, beside)

    def weights_along(n):
        return pltpu.make_async_remote_copy(
            src_ref=wrel.at[:, 0, :, my_lanes], dst_ref=wrel.at[:, 4 - n, :, my_lanes],
            send_sem=w1_send.at[n], recv_sem=w1_recv.at[4 - n],
            device_id=(j, 2 * ahead(4 * n) + k), device_id_type=MESH,
        )

    def weights_there(n):
        return pltpu.make_async_remote_copy(
            src_ref=wrel.at[:, 0, :, my_lanes], dst_ref=wrel.at[:, n, :, my_lanes],
            send_sem=w1_send.at[n], recv_sem=w1_recv.at[n],
            device_id=(j, 2 * ahead(4 * n) + k), device_id_type=MESH,
        )

    def small_along(n):
        return pltpu.make_async_remote_copy(
            src_ref=small_msg, dst_ref=small_got.at[quarter],
            send_sem=b_send.at[n], recv_sem=b_recv.at[4 - n],
            device_id=(j, 2 * ahead(4 * n) + k), device_id_type=MESH,
        )

    def weights_across(o):
        return pltpu.make_async_remote_copy(
            src_ref=wrel.at[:, pl.ds(1, 3), :, my_lanes], dst_ref=wrel.at[:, pl.ds(1, 3), :, my_lanes],
            send_sem=w2_send.at[o], recv_sem=w2_recv.at[o],
            device_id=(at_sp(o // 4, o % 4), t), device_id_type=MESH,
        )

    def send_block(source, src_z, dst_z, sem):
        return pltpu.make_async_remote_copy(
            src_ref=source, dst_ref=xt.at[rows_of(src_z, k), :], send_sem=sem, recv_sem=z_recv.at[src_z],
            device_id=(j, 2 * dst_z + k), device_id_type=MESH,
        )

    nxt, opp, prv = lax.rem(quarter + 1, 4), lax.rem(quarter + 2, 4), lax.rem(quarter + 3, 4)
    own_sends = [
        send_block(xs.at[:, group_of(quarter)], z, ahead(1), z_send.at[0]),
        send_block(xs.at[:, group_of(quarter)], z, ahead(N_Z - 1), z_send.at[1]),
        send_block(xs.at[:, group_of(nxt)], z, 4 * nxt, z_send.at[2]),
        send_block(xs.at[:, group_of(prv)], z, 4 * prv + 3, z_send.at[3]),
        send_block(xs.at[:, group_of(opp)], z, 4 * opp + jnp.where(i >= 2, 0, 3), z_send.at[4]),
    ]
    for n in (2, 1, 3):
        weights_along(n).start()

    @pl.when(i < 3)
    def _():
        own_sends[0].start()

    @pl.when(i > 0)
    def _():
        own_sends[1].start()

    for send in own_sends[2:]:
        send.start()

    def to_core(src_z, way, n):
        place = xt.at[rows_of(src_z, k), :]
        return pltpu.make_async_remote_copy(
            src_ref=place, dst_ref=place, send_sem=c_send.at[way, n], recv_sem=c_recv.at[way, n],
            device_id=(j, sibling), device_id_type=MESH,
        )

    to_core(z, 0, STEPS).start()
    for n in (2, 1, 3):
        small_along(n).start()
    small_got[quarter] = small_msg[...]
    for load in loads[7:]:
        load.wait()

    def behind(way):
        return i if way == 0 else 3 - i

    def source(way, n):
        e = n - behind(way)
        if way == 0:
            outside = jnp.where(e < 4, 4 * prv + 3 - e, 4 * opp + 7 - e)
            return jnp.where(e < 0, lax.rem(z - (n + 1) + 2 * N_Z, N_Z), outside)
        outside = jnp.where(e < 4, 4 * nxt + e, 4 * opp + e - 4)
        return jnp.where(e < 0, lax.rem(z + n + 1, N_Z), outside)

    def when_due(way, n, action):
        pl.when((n >= 0) & (n < 6 + behind(way)))(action)

    def onward(way, n):
        src = source(way, n)
        return send_block(xt.at[rows_of(src, k), :], src, ahead(1 if way == 0 else N_Z - 1), f_send.at[way, n])

    def goes_on(way):
        return i < 3 if way == 0 else i > 0

    def take(way, n):
        def action():
            src = source(way, n)
            place = xt.at[rows_of(src, k), :]
            pltpu.make_async_remote_copy(
                src_ref=place, dst_ref=place, send_sem=f_send.at[way, n], recv_sem=z_recv.at[src],
                device_id=(j, sibling), device_id_type=MESH,
            ).wait_recv()

            @pl.when(goes_on(way))
            def _():
                onward(way, n).start()

            to_core(src, way, n).start()

        when_due(way, n, action)

    def feats_of(src_z):
        return pl.ds(pl.multiple_of(src_z * 2 * FEATS, 2 * FEATS), 2 * FEATS)

    def compute(src_z, first=False):
        wide = xt[feats_of(src_z), :].astype(jnp.float32)
        sq = jnp.sum((wide * wide).reshape(2 * FEATS // 8, 8, ROWS), axis=0)
        if first:
            squares[...] = sq
        else:
            squares[...] += sq

    def prepare(n):
        feats = pl.ds(256 * n, 256)
        wvt[:, feats] = (wv_ref[feats, :].astype(jnp.float32).T * gain_ref[:, feats]).astype(jnp.bfloat16)

    def process(way, n):
        def action():
            src = source(way, n)
            to_core(src, way, n).wait_recv()
            compute(src)

        when_due(way, n, action)

    for n in range(BEATS):
        for way in range(2):
            take(way, n - LAG * behind(way))
        if n == 0:
            to_core(z, 0, STEPS).wait_recv()
            compute(z, True)
        if n >= DEFER:
            for way in range(2):
                process(way, n - DEFER - LAG * behind(way))
        if n < MODEL // 256:
            prepare(n)
        if n in (2, 3, 4):
            phase = n - 2
            pl.semaphore_wait(near_sem.at[phase], 2)
            if phase < 2:
                pass_on(phase + 1, across)
        if n == WEIGHT_BEAT:
            for m in range(1, 4):
                weights_there(m).wait_recv()
            for o in SP_ORDER:
                weights_across(o).start()
    for n in range(1, 4):
        small_along(n).wait_recv()
    bias = jnp.concatenate([column_of(small_got[b, 0:1, 0:CH]) for b in range(4)], axis=0)
    q_rows = jnp.concatenate([small_got[b, 1:2, 0:CH] for b in range(4)] + [jnp.zeros((4, CH), jnp.float32)], axis=0)
    q_row = lane_row(q_rows)
    og_row = lane_row(jnp.concatenate([og_ref[...], jnp.zeros((4, VT), jnp.float32)], axis=0))
    row_at = lax.broadcasted_iota(jnp.int32, (128, 256), 0)
    col_at = lax.broadcasted_iota(jnp.int32, (128, 256), 1)
    summing = jnp.where((row_at > col_at) | (col_at >= 128), 1.0, 0.0).astype(jnp.bfloat16)
    for o in SP_ORDER:
        weights_across(o).wait_recv()
    for n in range(BEATS - DEFER, BEATS):
        for way in range(2):
            process(way, n - LAG * behind(way))

    inverse = lax.rsqrt(jnp.sum(squares[...], axis=0, keepdims=True) * (1.0 / MODEL) + EPS)
    gate = jnp.dot(wrel[1].reshape(NCH, MODEL), xt[...], preferred_element_type=jnp.float32)
    gate = (gate * inverse).astype(jnp.bfloat16).astype(jnp.float32)
    for m in range(4):
        gate_scr[lax.rem(quarter + m, 4)] = gate[CH * m : CH * m + CH]
    u = gate_scr[...].reshape(NCH, ROWS) + bias + drift_ref[:, group_of(quarter)]
    log_decay = (jnp.minimum(u, 0.0) - jnp.log1p(jnp.exp(-jnp.abs(u)))) * (1.0 / GATE_NORM)
    blocks = ROWS // 128
    stacked = jnp.concatenate([log_decay[:, 128 * b : 128 * b + 128] for b in range(blocks)], axis=0)
    high = stacked.astype(jnp.bfloat16)
    left = stacked - high.astype(jnp.float32)
    mid = left.astype(jnp.bfloat16)
    low = (left - mid.astype(jnp.float32)).astype(jnp.bfloat16)
    summed = (
        jnp.dot(low, summing, preferred_element_type=jnp.float32)
        + jnp.dot(mid, summing, preferred_element_type=jnp.float32)
        + jnp.dot(high, summing, preferred_element_type=jnp.float32)
    )
    rests = [None] * blocks
    run = jnp.zeros((NCH, 128), jnp.float32)
    for b in reversed(range(blocks)):
        rests[b] = summed[NCH * b : NCH * b + NCH, 0:128] + run
        run = run + summed[NCH * b : NCH * b + NCH, 128:256]
    d_msg[...] = run.T[0:1, :]

    def decays(o):
        return pltpu.make_async_remote_copy(
            src_ref=d_msg, dst_ref=d_got.at[4 * j + quarter], send_sem=d_send.at[o], recv_sem=d_recv.at[o],
            device_id=(at_sp((o % 16) // 4, o % 4), 2 * ahead(4 * (o // 16)) + k), device_id_type=MESH,
        )

    for o in ALL_ORDER:
        decays(o).start()
    d_got[4 * j + quarter] = d_msg[...]
    key = jnp.dot(wrel[0].reshape(NCH, MODEL), xt[...], preferred_element_type=jnp.float32)
    key = (key * inverse).astype(jnp.bfloat16).astype(jnp.float32)
    for m in range(4):
        key_scr[lax.rem(quarter + m, 4)] = key[CH * m : CH * m + CH]
    key = key_scr[...].reshape(NCH, ROWS)
    weighted = jnp.concatenate(
        [(key[:, 128 * b : 128 * b + 128] * jnp.exp(rests[b])).astype(jnp.bfloat16) for b in range(blocks)], axis=1
    )
    value = jnp.dot(wvt[...], xt[...], preferred_element_type=jnp.float32)
    value = (value * inverse).astype(jnp.bfloat16)
    partial = lax.dot_general(value, weighted, (((1,), (1,)), ((), ())), preferred_element_type=jnp.float32)
    msg[...] = partial.reshape(N_SP, VT, NCH)

    def exchange(o):
        to = at_sp(o // 4, o % 4)
        return pltpu.make_async_remote_copy(
            src_ref=msg.at[to], dst_ref=got.at[j], send_sem=p_send.at[o], recv_sem=p_recv.at[o],
            device_id=(to, t), device_id_type=MESH,
        )

    for o in SP_ORDER:
        exchange(o).start()
    got[j] = msg[j]

    for way in range(2):
        for n in range(STEPS):
            def action(way=way, n=n):
                @pl.when(goes_on(way))
                def _():
                    onward(way, n).wait_send()

                to_core(source(way, n), way, n).wait_send()

            when_due(way, n, action)
    to_core(z, 0, STEPS).wait_send()

    @pl.when(i < 3)
    def _():
        own_sends[0].wait_send()

    @pl.when(i > 0)
    def _():
        own_sends[1].wait_send()

    for send in own_sends[2:]:
        send.wait_send()
    for n in range(1, 4):
        weights_along(n).wait_send()
        small_along(n).wait_send()
    for o in SP_ORDER:
        weights_across(o).wait_send()

    for o in SP_ORDER:
        exchange(o).wait_recv()
    for o in reversed(ALL_ORDER):
        decays(o).wait_recv()
    later = jnp.zeros((1, NCH), jnp.float32)
    state = jnp.zeros((VT, NCH), jnp.float32)
    for n in reversed(range(N_SP)):
        mine = later
        for g in range(4):
            piece = d_got[4 * n + g]
            mine = mine + jnp.where(g > quarter, piece, 0.0)
            later = later + piece
        state = state + jnp.exp(mine) * got[n]
    lane_head = lax.broadcasted_iota(jnp.int32, (8, 128), 1) // VT
    pick_head = jnp.where(lane_head == lax.broadcasted_iota(jnp.int32, (8, 128), 0), 1.0, 0.0)
    head_rows = lax.dot_general(
        pick_head, state * q_row, (((1,), (1,)), ((), ())), precision=HIGH, preferred_element_type=jnp.float32
    )
    read_msg[...] = lane_row(head_rows)

    def tell(o):
        return pltpu.make_async_remote_copy(
            src_ref=read_msg, dst_ref=read_got.at[t], send_sem=r_send.at[o], recv_sem=r_recv.at[o],
            device_id=(j, 2 * ahead(o // 2) + lax.rem(k + o % 2, 2)), device_id_type=MESH,
        )

    for o in TP_ORDER:
        tell(o).start()
    st_got[0] = state

    def states(n):
        return pltpu.make_async_remote_copy(
            src_ref=st_got.at[0], dst_ref=st_got.at[4 - n], send_sem=t_send.at[n], recv_sem=t_recv.at[4 - n],
            device_id=(j, 2 * ahead(4 * n) + k), device_id_type=MESH,
        )

    for n in (2, 1, 3):
        states(n).start()
    read_got[t] = read_msg[...]
    for o in SP_ORDER:
        exchange(o).wait_send()
    for o in ALL_ORDER:
        decays(o).wait_send()
    for o in TP_ORDER:
        tell(o).wait_recv()
    read = read_got[0]
    for n in range(1, N_TP):
        read = read + read_got[n]
    lane_group = lax.broadcasted_iota(jnp.int32, (1, 128), 1) // VT
    sq = jnp.zeros((1, 128), jnp.float32)
    for h in range(HEADS):
        own = jnp.sum(jnp.where(lane_group == h, read * read, 0.0), axis=1, keepdims=True)
        sq = jnp.where(lane_group == h, jnp.broadcast_to(own, (1, 128)), sq)
    sq_msg[...] = sq

    def share(o):
        return pltpu.make_async_remote_copy(
            src_ref=sq_msg, dst_ref=sq_got.at[j], send_sem=s_send.at[o], recv_sem=s_recv.at[o],
            device_id=(at_sp(o // 4, o % 4), t), device_id_type=MESH,
        )

    for o in SP_ORDER:
        share(o).start()
    sq_got[j] = sq_msg[...]
    for n in range(1, 4):
        states(n).wait_recv()
    total = st_got[0] + st_got[1] + st_got[2] + st_got[3]
    turned[...] = jnp.concatenate([total] * 4, axis=0).T
    out_ref[0:CH, :] = turned[pl.ds(pl.multiple_of(CH * quarter, CH), CH), :]
    for n in range(1, 4):
        states(n).wait_send()
    for o in TP_ORDER:
        tell(o).wait_send()
    for o in SP_ORDER:
        share(o).wait_recv()
    whole = sq_got[0]
    for n in range(1, N_SP):
        whole = whole + sq_got[n]
    out_ref[CH : CH + 1, :] = read * lax.rsqrt(whole * (1.0 / VALS) + EPS) * og_row
    for o in SP_ORDER:
        share(o).wait_send()


def unpack(packed_ref, state_ref, read_ref):
    state_ref[...] = packed_ref[0:CH, 0:VT].astype(jnp.bfloat16)
    for h in range(HEADS):
        read_ref[h : h + 1, :] = packed_ref[CH : CH + 1, VT * h : VT * h + VT]


def body(tokens, norm_gain, w_key, w_decay, w_value, decay_bias, gate_drift, queries, out_gain):
    dma = pltpu.SemaphoreType.DMA
    vmem = pl.BlockSpec(memory_space=pltpu.VMEM)
    f32, bf16 = jnp.float32, jnp.bfloat16
    packed = pl.pallas_call(
        kernel,
        out_shape=jax.ShapeDtypeStruct((CH + 8, 128), f32),
        in_specs=[pl.BlockSpec(memory_space=pl.ANY)] * 9,
        out_specs=vmem,
        scratch_shapes=[
            pltpu.VMEM((FEATS, SPAN), bf16),
            pltpu.VMEM((MODEL, ROWS), bf16),
            pltpu.VMEM((1, MODEL), f32),
            pltpu.VMEM((CH, MODEL), bf16),
            pltpu.VMEM((CH, MODEL), bf16),
            pltpu.VMEM((MODEL, VALS), bf16),
            pltpu.VMEM((1, CH), f32),
            pltpu.VMEM((1, SPAN), f32),
            pltpu.VMEM((1, CH), bf16),
            pltpu.VMEM((HEADS, VT), f32),
            pltpu.VMEM((2, 4, CH, MODEL), bf16),
            pltpu.VMEM((VALS, MODEL), bf16),
            pltpu.VMEM((8, ROWS), f32),
            pltpu.VMEM((2, 128), f32),
            pltpu.VMEM((4, 2, 128), f32),
            pltpu.VMEM((4, CH, ROWS), f32),
            pltpu.VMEM((4, CH, ROWS), f32),
            pltpu.VMEM((N_SP, VT, NCH), f32),
            pltpu.VMEM((N_SP, VT, NCH), f32),
            pltpu.VMEM((1, 128), f32),
            pltpu.VMEM((4 * N_SP, 1, 128), f32),
            pltpu.VMEM((1, 128), f32),
            pltpu.VMEM((N_TP, 1, 128), f32),
            pltpu.VMEM((1, 128), f32),
            pltpu.VMEM((N_SP, 1, 128), f32),
            pltpu.VMEM((4, VT, NCH), f32),
            pltpu.VMEM((128, 128), f32),
            pltpu.SemaphoreType.REGULAR((3,)), dma((10,)), dma((5,)), dma((N_Z,)), dma((2, STEPS)),
            dma((2, STEPS + 1)), dma((2, STEPS + 1)), dma((4,)), dma((4,)), dma((N_SP,)), dma((N_SP,)), dma((4,)), dma((4,)),
            dma((64,)), dma((64,)), dma((N_SP,)), dma((N_SP,)), dma((N_TP,)), dma((N_TP,)), dma((4,)), dma((4,)),
            dma((N_SP,)), dma((N_SP,)),
        ],
        compiler_params=pltpu.CompilerParams(
            collective_id=0, has_side_effects=True, vmem_limit_bytes=67043328
        ),
    )(
        tokens.T, norm_gain.reshape(1, MODEL), w_key.T, w_decay.T, w_value, decay_bias.reshape(1, CH),
        gate_drift.reshape(1, SPAN), queries.reshape(1, CH), out_gain,
    )
    return pl.pallas_call(
        unpack,
        out_shape=(jax.ShapeDtypeStruct((CH, VT), bf16), jax.ShapeDtypeStruct((HEADS, VT), f32)),
        in_specs=[vmem],
        out_specs=(vmem, vmem),
    )(packed)


def solution(mesh):
    return jax.shard_map(
        body,
        mesh=mesh,
        in_specs=(
            P("sp", "tp"), P(), P(None, "tp"), P(None, "tp"), P(), P("tp"), P("sp"), P("tp"), P(None, "sp"),
        ),
        out_specs=(P("tp", "sp"), P(None, "sp")),
        check_vma=False,
    )
```

```python
import jax
import jax.numpy as jnp
from jax import lax
from jax.experimental import pallas as pl
from jax.experimental.pallas import tpu as pltpu
from jax.sharding import PartitionSpec as P

MESH = pl.DeviceIdType.MESH
EPS = 1e-06
GATE_NORM = 16.0
KEY_CHANNELS = 256
N_SP, N_TP, N_Z = 16, 32, 16
SPAN, FEATS, VALS, CH = 2048, 64, 512, 32
QUARTERS = 4
ROWS = SPAN // QUARTERS
NCH = QUARTERS * CH
VT = 32
HEADS = 4
MODEL = N_TP * FEATS
STEPS = 9
LAG = 2
DEFER = 2
BEATS = 9 + 3 * LAG
WEIGHT_BEAT = 3
HIGH = lax.Precision.HIGHEST


def hops(step, size):
    return min(step, size - step)


def sp_hops(o):
    return hops(o // 4, 4) + hops(o % 4, 4)


SP_ORDER = sorted(range(1, N_SP), key=lambda o: -sp_hops(o))
TP_ORDER = sorted(range(1, N_TP), key=lambda o: -hops(o // 2, N_Z))
ALL_ORDER = sorted(range(1, 4 * N_SP), key=lambda o: -(hops(4 * (o // 16), N_Z) + sp_hops(o % 16)))


def column_of(row):
    n = row.shape[1]
    on_diagonal = lax.broadcasted_iota(jnp.int32, (n, n), 0) == lax.broadcasted_iota(jnp.int32, (n, n), 1)
    return jnp.sum(jnp.where(on_diagonal, jnp.broadcast_to(row, (n, n)), 0.0), axis=1, keepdims=True)


def lane_row(rows):
    at = lax.broadcasted_iota(jnp.int32, (VT, 128), 1)
    pick = jnp.where(lax.rem(at, VT) == lax.broadcasted_iota(jnp.int32, (VT, 128), 0), 1.0, 0.0)
    wide = jnp.dot(rows, pick, precision=HIGH, preferred_element_type=jnp.float32)
    lane = lax.broadcasted_iota(jnp.int32, (8, 128), 1) // VT
    mine = lane == lax.broadcasted_iota(jnp.int32, (8, 128), 0)
    return jnp.sum(jnp.where(mine, wide, 0.0), axis=0, keepdims=True)


def kernel(
    x_hbm, gain_hbm, wk_hbm, wd_hbm, wv_hbm, bias_hbm, drift_hbm, q_hbm, og_hbm,
    out_ref,
    xs, xt, gain_ref, wk_ref, wd_ref, wv_ref, bias_ref, drift_ref, q_ref, og_ref,
    wrel, wvt, squares, small_msg, small_got, key_scr, gate_scr, msg, got, d_msg, d_got,
    read_msg, read_got, sq_msg, sq_got, st_got, turned,
    near_sem, in_sem, z_send, z_recv, f_send, c_send, c_recv, w1_send, w1_recv, w2_send, w2_recv, b_send, b_recv,
    d_send, d_recv, p_send, p_recv, r_send, r_recv, t_send, t_recv, s_send, s_recv,
):
    j = lax.axis_index("sp")
    t = lax.axis_index("tp")
    z, k = t // 2, t % 2
    quarter, i = z // 4, z % 4
    y, x = j // 4, j % 4
    sibling = 2 * z + 1 - k

    def at_sp(dy, dx):
        return lax.rem(y + dy, 4) * 4 + lax.rem(x + dx, 4)

    def ahead(dz):
        return lax.rem(z + dz, N_Z)

    barrier = pltpu.get_barrier_semaphore()
    pl.semaphore_signal(barrier, inc=1, device_id=(j, sibling), device_id_type=MESH)
    beside = (at_sp(0, 1), at_sp(0, 3))
    across = (at_sp(1, 0), at_sp(3, 0))
    for other in beside + across:
        pl.semaphore_signal(barrier, inc=1, device_id=(other, t), device_id_type=MESH)
    for dz in range(1, N_Z):
        pl.semaphore_signal(barrier, inc=1, device_id=(j, 2 * ahead(dz) + k), device_id_type=MESH)

    def rows_of(src_z, core):
        return pl.ds(pl.multiple_of((2 * src_z + core) * FEATS, FEATS), FEATS)

    def group_of(q):
        return pl.ds(pl.multiple_of(q * ROWS, ROWS), ROWS)

    my_lanes = pl.ds(pl.multiple_of(j * 128, 128), 128)

    loads = [
        pltpu.make_async_copy(src, dst, in_sem.at[n])
        for n, (src, dst) in enumerate(
            [
                (x_hbm, xs), (gain_hbm, gain_ref), (wk_hbm, wk_ref), (wd_hbm, wd_ref), (bias_hbm, bias_ref),
                (q_hbm, q_ref), (x_hbm.at[:, group_of(quarter)], xt.at[rows_of(z, k), :]),
                (wv_hbm, wv_ref), (drift_hbm, drift_ref), (og_hbm, og_ref),
            ]
        )
    ]
    for load in loads:
        load.start()
    for load in loads[:7]:
        load.wait()
    gain = gain_ref[...]
    wrel[0, 0] = (wk_ref[...].astype(jnp.float32) * gain).astype(jnp.bfloat16)
    wrel[1, 0] = (wd_ref[...].astype(jnp.float32) * gain).astype(jnp.bfloat16)
    small_msg[...] = jnp.zeros((2, 128), jnp.float32)
    small_msg[0:1, 0:CH] = bias_ref[...]
    small_msg[1:2, 0:CH] = q_ref[...].astype(jnp.float32) * KEY_CHANNELS ** (-0.5)
    pl.semaphore_wait(barrier, 5 + N_Z - 1)

    def pass_on(phase, others):
        for other in others:
            pl.semaphore_signal(near_sem.at[phase], inc=1, device_id=(other, t), device_id_type=MESH)

    pass_on(0, beside)

    def weights_along(n):
        return pltpu.make_async_remote_copy(
            src_ref=wrel.at[:, 0, :, my_lanes], dst_ref=wrel.at[:, 4 - n, :, my_lanes],
            send_sem=w1_send.at[n], recv_sem=w1_recv.at[4 - n],
            device_id=(j, 2 * ahead(4 * n) + k), device_id_type=MESH,
        )

    def weights_there(n):
        return pltpu.make_async_remote_copy(
            src_ref=wrel.at[:, 0, :, my_lanes], dst_ref=wrel.at[:, n, :, my_lanes],
            send_sem=w1_send.at[n], recv_sem=w1_recv.at[n],
            device_id=(j, 2 * ahead(4 * n) + k), device_id_type=MESH,
        )

    def small_along(n):
        return pltpu.make_async_remote_copy(
            src_ref=small_msg, dst_ref=small_got.at[quarter],
            send_sem=b_send.at[n], recv_sem=b_recv.at[4 - n],
            device_id=(j, 2 * ahead(4 * n) + k), device_id_type=MESH,
        )

    def weights_across(o):
        return pltpu.make_async_remote_copy(
            src_ref=wrel.at[:, pl.ds(1, 3), :, my_lanes], dst_ref=wrel.at[:, pl.ds(1, 3), :, my_lanes],
            send_sem=w2_send.at[o], recv_sem=w2_recv.at[o],
            device_id=(at_sp(o // 4, o % 4), t), device_id_type=MESH,
        )

    def send_block(source, src_z, dst_z, sem):
        return pltpu.make_async_remote_copy(
            src_ref=source, dst_ref=xt.at[rows_of(src_z, k), :], send_sem=sem, recv_sem=z_recv.at[src_z],
            device_id=(j, 2 * dst_z + k), device_id_type=MESH,
        )

    nxt, opp, prv = lax.rem(quarter + 1, 4), lax.rem(quarter + 2, 4), lax.rem(quarter + 3, 4)
    own_sends = [
        send_block(xs.at[:, group_of(quarter)], z, ahead(1), z_send.at[0]),
        send_block(xs.at[:, group_of(quarter)], z, ahead(N_Z - 1), z_send.at[1]),
        send_block(xs.at[:, group_of(nxt)], z, 4 * nxt, z_send.at[2]),
        send_block(xs.at[:, group_of(prv)], z, 4 * prv + 3, z_send.at[3]),
        send_block(xs.at[:, group_of(opp)], z, 4 * opp + jnp.where(i >= 2, 0, 3), z_send.at[4]),
    ]
    for n in (2, 1, 3):
        weights_along(n).start()

    @pl.when(i < 3)
    def _():
        own_sends[0].start()

    @pl.when(i > 0)
    def _():
        own_sends[1].start()

    for send in own_sends[2:]:
        send.start()

    def to_core(src_z, way, n):
        place = xt.at[rows_of(src_z, k), :]
        return pltpu.make_async_remote_copy(
            src_ref=place, dst_ref=place, send_sem=c_send.at[way, n], recv_sem=c_recv.at[way, n],
            device_id=(j, sibling), device_id_type=MESH,
        )

    to_core(z, 0, STEPS).start()
    for n in (2, 1, 3):
        small_along(n).start()
    small_got[quarter] = small_msg[...]
    for load in loads[7:]:
        load.wait()

    def behind(way):
        return i if way == 0 else 3 - i

    def source(way, n):
        e = n - behind(way)
        if way == 0:
            outside = jnp.where(e < 4, 4 * prv + 3 - e, 4 * opp + 7 - e)
            return jnp.where(e < 0, lax.rem(z - (n + 1) + 2 * N_Z, N_Z), outside)
        outside = jnp.where(e < 4, 4 * nxt + e, 4 * opp + e - 4)
        return jnp.where(e < 0, lax.rem(z + n + 1, N_Z), outside)

    def when_due(way, n, action):
        pl.when((n >= 0) & (n < 6 + behind(way)))(action)

    def onward(way, n):
        src = source(way, n)
        return send_block(xt.at[rows_of(src, k), :], src, ahead(1 if way == 0 else N_Z - 1), f_send.at[way, n])

    def goes_on(way):
        return i < 3 if way == 0 else i > 0

    def take(way, n):
        def action():
            src = source(way, n)
            place = xt.at[rows_of(src, k), :]
            pltpu.make_async_remote_copy(
                src_ref=place, dst_ref=place, send_sem=f_send.at[way, n], recv_sem=z_recv.at[src],
                device_id=(j, sibling), device_id_type=MESH,
            ).wait_recv()

            @pl.when(goes_on(way))
            def _():
                onward(way, n).start()

            to_core(src, way, n).start()

        when_due(way, n, action)

    def feats_of(src_z):
        return pl.ds(pl.multiple_of(src_z * 2 * FEATS, 2 * FEATS), 2 * FEATS)

    def compute(src_z, first=False):
        wide = xt[feats_of(src_z), :].astype(jnp.float32)
        sq = jnp.sum((wide * wide).reshape(2 * FEATS // 8, 8, ROWS), axis=0)
        if first:
            squares[...] = sq
        else:
            squares[...] += sq

    def prepare(n):
        feats = pl.ds(256 * n, 256)
        wvt[:, feats] = (wv_ref[feats, :].astype(jnp.float32).T * gain_ref[:, feats]).astype(jnp.bfloat16)

    def process(way, n):
        def action():
            src = source(way, n)
            to_core(src, way, n).wait_recv()
            compute(src)

        when_due(way, n, action)

    for n in range(BEATS):
        for way in range(2):
            take(way, n - LAG * behind(way))
        if n == 0:
            to_core(z, 0, STEPS).wait_recv()
            compute(z, True)
        if n >= DEFER:
            for way in range(2):
                process(way, n - DEFER - LAG * behind(way))
        if n < MODEL // 256:
            prepare(n)
        if n in (0, 1, 2):
            phase = n
            pl.semaphore_wait(near_sem.at[phase], 2)
            if phase < 2:
                pass_on(phase + 1, across)
        if n == WEIGHT_BEAT:
            for m in range(1, 4):
                weights_there(m).wait_recv()
            for o in SP_ORDER:
                weights_across(o).start()
    for n in range(1, 4):
        small_along(n).wait_recv()
    bias = jnp.concatenate([column_of(small_got[b, 0:1, 0:CH]) for b in range(4)], axis=0)
    q_rows = jnp.concatenate([small_got[b, 1:2, 0:CH] for b in range(4)] + [jnp.zeros((4, CH), jnp.float32)], axis=0)
    q_row = lane_row(q_rows)
    og_row = lane_row(jnp.concatenate([og_ref[...], jnp.zeros((4, VT), jnp.float32)], axis=0))
    row_at = lax.broadcasted_iota(jnp.int32, (128, 256), 0)
    col_at = lax.broadcasted_iota(jnp.int32, (128, 256), 1)
    summing = jnp.where((row_at > col_at) | (col_at >= 128), 1.0, 0.0).astype(jnp.bfloat16)
    for o in SP_ORDER:
        weights_across(o).wait_recv()
    for n in range(BEATS - DEFER, BEATS):
        for way in range(2):
            process(way, n - LAG * behind(way))

    inverse = lax.rsqrt(jnp.sum(squares[...], axis=0, keepdims=True) * (1.0 / MODEL) + EPS)
    gate = jnp.dot(wrel[1].reshape(NCH, MODEL), xt[...], preferred_element_type=jnp.float32)
    gate = (gate * inverse).astype(jnp.bfloat16).astype(jnp.float32)
    for m in range(4):
        gate_scr[lax.rem(quarter + m, 4)] = gate[CH * m : CH * m + CH]
    u = gate_scr[...].reshape(NCH, ROWS) + bias + drift_ref[:, group_of(quarter)]
    log_decay = (jnp.minimum(u, 0.0) - jnp.log1p(jnp.exp(-jnp.abs(u)))) * (1.0 / GATE_NORM)
    blocks = ROWS // 128
    stacked = jnp.concatenate([log_decay[:, 128 * b : 128 * b + 128] for b in range(blocks)], axis=0)
    high = stacked.astype(jnp.bfloat16)
    left = stacked - high.astype(jnp.float32)
    mid = left.astype(jnp.bfloat16)
    low = (left - mid.astype(jnp.float32)).astype(jnp.bfloat16)
    summed = (
        jnp.dot(low, summing, preferred_element_type=jnp.float32)
        + jnp.dot(mid, summing, preferred_element_type=jnp.float32)
        + jnp.dot(high, summing, preferred_element_type=jnp.float32)
    )
    rests = [None] * blocks
    run = jnp.zeros((NCH, 128), jnp.float32)
    for b in reversed(range(blocks)):
        rests[b] = summed[NCH * b : NCH * b + NCH, 0:128] + run
        run = run + summed[NCH * b : NCH * b + NCH, 128:256]
    d_msg[...] = run.T[0:1, :]

    def decays(o):
        return pltpu.make_async_remote_copy(
            src_ref=d_msg, dst_ref=d_got.at[4 * j + quarter], send_sem=d_send.at[o], recv_sem=d_recv.at[o],
            device_id=(at_sp((o % 16) // 4, o % 4), 2 * ahead(4 * (o // 16)) + k), device_id_type=MESH,
        )

    for o in ALL_ORDER:
        decays(o).start()
    d_got[4 * j + quarter] = d_msg[...]
    key = jnp.dot(wrel[0].reshape(NCH, MODEL), xt[...], preferred_element_type=jnp.float32)
    key = (key * inverse).astype(jnp.bfloat16).astype(jnp.float32)
    for m in range(4):
        key_scr[lax.rem(quarter + m, 4)] = key[CH * m : CH * m + CH]
    key = key_scr[...].reshape(NCH, ROWS)
    weighted = jnp.concatenate(
        [(key[:, 128 * b : 128 * b + 128] * jnp.exp(rests[b])).astype(jnp.bfloat16) for b in range(blocks)], axis=1
    )
    value = jnp.dot(wvt[...], xt[...], preferred_element_type=jnp.float32)
    value = (value * inverse).astype(jnp.bfloat16)
    partial = lax.dot_general(value, weighted, (((1,), (1,)), ((), ())), preferred_element_type=jnp.float32)
    msg[...] = partial.astype(jnp.bfloat16).reshape(N_SP, VT, NCH)

    def exchange(o):
        to = at_sp(o // 4, o % 4)
        return pltpu.make_async_remote_copy(
            src_ref=msg.at[to], dst_ref=got.at[j], send_sem=p_send.at[o], recv_sem=p_recv.at[o],
            device_id=(to, t), device_id_type=MESH,
        )

    for o in SP_ORDER:
        exchange(o).start()
    got[j] = msg[j]

    for way in range(2):
        for n in range(STEPS):
            def action(way=way, n=n):
                @pl.when(goes_on(way))
                def _():
                    onward(way, n).wait_send()

                to_core(source(way, n), way, n).wait_send()

            when_due(way, n, action)
    to_core(z, 0, STEPS).wait_send()

    @pl.when(i < 3)
    def _():
        own_sends[0].wait_send()

    @pl.when(i > 0)
    def _():
        own_sends[1].wait_send()

    for send in own_sends[2:]:
        send.wait_send()
    for n in range(1, 4):
        weights_along(n).wait_send()
        small_along(n).wait_send()
    for o in SP_ORDER:
        weights_across(o).wait_send()

    for o in SP_ORDER:
        exchange(o).wait_recv()
    for o in reversed(ALL_ORDER):
        decays(o).wait_recv()
    later = jnp.zeros((1, NCH), jnp.float32)
    state = jnp.zeros((VT, NCH), jnp.float32)
    for n in reversed(range(N_SP)):
        mine = later
        for g in range(4):
            piece = d_got[4 * n + g]
            mine = mine + jnp.where(g > quarter, piece, 0.0)
            later = later + piece
        state = state + jnp.exp(mine) * got[n].astype(jnp.float32)
    lane_head = lax.broadcasted_iota(jnp.int32, (8, 128), 1) // VT
    pick_head = jnp.where(lane_head == lax.broadcasted_iota(jnp.int32, (8, 128), 0), 1.0, 0.0)
    head_rows = lax.dot_general(
        pick_head, state * q_row, (((1,), (1,)), ((), ())), precision=HIGH, preferred_element_type=jnp.float32
    )
    read_msg[...] = lane_row(head_rows)

    def tell(o):
        return pltpu.make_async_remote_copy(
            src_ref=read_msg, dst_ref=read_got.at[t], send_sem=r_send.at[o], recv_sem=r_recv.at[o],
            device_id=(j, 2 * ahead(o // 2) + lax.rem(k + o % 2, 2)), device_id_type=MESH,
        )

    for o in TP_ORDER:
        tell(o).start()
    st_got[0] = state

    def states(n):
        return pltpu.make_async_remote_copy(
            src_ref=st_got.at[0], dst_ref=st_got.at[4 - n], send_sem=t_send.at[n], recv_sem=t_recv.at[4 - n],
            device_id=(j, 2 * ahead(4 * n) + k), device_id_type=MESH,
        )

    for n in (2, 1, 3):
        states(n).start()
    read_got[t] = read_msg[...]
    for o in SP_ORDER:
        exchange(o).wait_send()
    for o in ALL_ORDER:
        decays(o).wait_send()
    for o in TP_ORDER:
        tell(o).wait_recv()
    read = read_got[0]
    for n in range(1, N_TP):
        read = read + read_got[n]
    lane_group = lax.broadcasted_iota(jnp.int32, (1, 128), 1) // VT
    sq = jnp.zeros((1, 128), jnp.float32)
    for h in range(HEADS):
        own = jnp.sum(jnp.where(lane_group == h, read * read, 0.0), axis=1, keepdims=True)
        sq = jnp.where(lane_group == h, jnp.broadcast_to(own, (1, 128)), sq)
    sq_msg[...] = sq

    def share(o):
        return pltpu.make_async_remote_copy(
            src_ref=sq_msg, dst_ref=sq_got.at[j], send_sem=s_send.at[o], recv_sem=s_recv.at[o],
            device_id=(at_sp(o // 4, o % 4), t), device_id_type=MESH,
        )

    for o in SP_ORDER:
        share(o).start()
    sq_got[j] = sq_msg[...]
    for n in range(1, 4):
        states(n).wait_recv()
    total = st_got[0] + st_got[1] + st_got[2] + st_got[3]
    turned[...] = jnp.concatenate([total] * 4, axis=0).T
    out_ref[0:CH, :] = turned[pl.ds(pl.multiple_of(CH * quarter, CH), CH), :]
    for n in range(1, 4):
        states(n).wait_send()
    for o in TP_ORDER:
        tell(o).wait_send()
    for o in SP_ORDER:
        share(o).wait_recv()
    whole = sq_got[0]
    for n in range(1, N_SP):
        whole = whole + sq_got[n]
    out_ref[CH : CH + 1, :] = read * lax.rsqrt(whole * (1.0 / VALS) + EPS) * og_row
    for o in SP_ORDER:
        share(o).wait_send()


def unpack(packed_ref, state_ref, read_ref):
    state_ref[...] = packed_ref[0:CH, 0:VT].astype(jnp.bfloat16)
    for h in range(HEADS):
        read_ref[h : h + 1, :] = packed_ref[CH : CH + 1, VT * h : VT * h + VT]


def body(tokens, norm_gain, w_key, w_decay, w_value, decay_bias, gate_drift, queries, out_gain):
    dma = pltpu.SemaphoreType.DMA
    vmem = pl.BlockSpec(memory_space=pltpu.VMEM)
    f32, bf16 = jnp.float32, jnp.bfloat16
    packed = pl.pallas_call(
        kernel,
        out_shape=jax.ShapeDtypeStruct((CH + 8, 128), f32),
        in_specs=[pl.BlockSpec(memory_space=pl.ANY)] * 9,
        out_specs=vmem,
        scratch_shapes=[
            pltpu.VMEM((FEATS, SPAN), bf16),
            pltpu.VMEM((MODEL, ROWS), bf16),
            pltpu.VMEM((1, MODEL), f32),
            pltpu.VMEM((CH, MODEL), bf16),
            pltpu.VMEM((CH, MODEL), bf16),
            pltpu.VMEM((MODEL, VALS), bf16),
            pltpu.VMEM((1, CH), f32),
            pltpu.VMEM((1, SPAN), f32),
            pltpu.VMEM((1, CH), bf16),
            pltpu.VMEM((HEADS, VT), f32),
            pltpu.VMEM((2, 4, CH, MODEL), bf16),
            pltpu.VMEM((VALS, MODEL), bf16),
            pltpu.VMEM((8, ROWS), f32),
            pltpu.VMEM((2, 128), f32),
            pltpu.VMEM((4, 2, 128), f32),
            pltpu.VMEM((4, CH, ROWS), f32),
            pltpu.VMEM((4, CH, ROWS), f32),
            pltpu.VMEM((N_SP, VT, NCH), bf16),
            pltpu.VMEM((N_SP, VT, NCH), bf16),
            pltpu.VMEM((1, 128), f32),
            pltpu.VMEM((4 * N_SP, 1, 128), f32),
            pltpu.VMEM((1, 128), f32),
            pltpu.VMEM((N_TP, 1, 128), f32),
            pltpu.VMEM((1, 128), f32),
            pltpu.VMEM((N_SP, 1, 128), f32),
            pltpu.VMEM((4, VT, NCH), f32),
            pltpu.VMEM((128, 128), f32),
            pltpu.SemaphoreType.REGULAR((3,)), dma((10,)), dma((5,)), dma((N_Z,)), dma((2, STEPS)),
            dma((2, STEPS + 1)), dma((2, STEPS + 1)), dma((4,)), dma((4,)), dma((N_SP,)), dma((N_SP,)), dma((4,)), dma((4,)),
            dma((64,)), dma((64,)), dma((N_SP,)), dma((N_SP,)), dma((N_TP,)), dma((N_TP,)), dma((4,)), dma((4,)),
            dma((N_SP,)), dma((N_SP,)),
        ],
        compiler_params=pltpu.CompilerParams(
            collective_id=0, has_side_effects=True, vmem_limit_bytes=67043328
        ),
    )(
        tokens.T, norm_gain.reshape(1, MODEL), w_key.T, w_decay.T, w_value, decay_bias.reshape(1, CH),
        gate_drift.reshape(1, SPAN), queries.reshape(1, CH), out_gain,
    )
    return pl.pallas_call(
        unpack,
        out_shape=(jax.ShapeDtypeStruct((CH, VT), bf16), jax.ShapeDtypeStruct((HEADS, VT), f32)),
        in_specs=[vmem],
        out_specs=(vmem, vmem),
    )(packed)


def solution(mesh):
    return jax.shard_map(
        body,
        mesh=mesh,
        in_specs=(
            P("sp", "tp"), P(), P(None, "tp"), P(None, "tp"), P(), P("tp"), P("sp"), P("tp"), P(None, "sp"),
        ),
        out_specs=(P("tp", "sp"), P(None, "sp")),
        check_vma=False,
    )
```
